32 devices in a mesh: ep: 8 (over z, y), tp: 4 (over x, core).
Axes of the slice: x: 2, y: 2, z: 4, core: 2. Of those that a mesh axis runs over, the one named last changes fastest.
Arguments:
- tokens: bfloat16 [2048, 2048], P('ep'), may hold values from -6 to 6
- expert_ids: int32 [2048, 2], P('ep'), may hold values from 0 to 7, all different within a row; in each aligned block of 256 rows (0 to 255, 256 to 511, ...) at most 192 rows name the same one
- route_weight: float32 [2048, 2], P('ep'), may hold values from 0.1 to 1
- norm_gain: float32 [2048], replicated, may hold values from 0.1 to 1.9
- expert_gate: bfloat16 [8, 2048, 2048], P('ep', None, 'tp'), may hold values from -4 to 4
- expert_up: bfloat16 [8, 2048, 2048], P('ep', None, 'tp'), may hold values from -4 to 4
- expert_down: bfloat16 [8, 2048, 2048], P('ep', 'tp'), may hold values from -0.03125 to 0.03125
Outputs:
- combined: bfloat16 [2048, 2048], P('ep', 'tp')
The draws below stay inside these ranges and needn't reach their ends.
Inputs may be any that keep to these rules, and one draw needn't show every extreme that they name: `expert_ids`: each row names 2 different experts. In each aligned block of 256 rows (the rows of one index of ep) no expert is named by more than 192 rows, and in some block one expert is named by exactly 192 rows.
All inputs are finite; a program needn't handle non-finite values.
Results may differ from the reference program's by a relative error of at most 0.012.
Values may be sent and summed in bfloat16 or wider, within the bound.
A program may use at most 128 MiB of HBM per device.

```python
import math
import jax
import jax.numpy as jnp
import numpy as np
from jax import lax

D = 2048
FF = 2048
TOP_K = 2
TOK_GROUP = 256
EXPERTS = 8
TOKENS = 2048
CAP = 192
N_EP = 8
N_TP = 4


def draw_expert_gate(key, part):
    spread = 3.0
    normal_draw = jax.random.truncated_normal(jax.random.fold_in(key, 11), -4.0, 4.0, (EXPERTS, D, FF), jnp.float32)
    return (normal_draw * (spread / math.sqrt(D))).astype(jnp.bfloat16)


def draw_expert_up(key, part):
    spread = 3.0
    normal_draw = jax.random.truncated_normal(jax.random.fold_in(key, 23), -4.0, 4.0, (EXPERTS, D, FF), jnp.float32)
    return (normal_draw * (spread / math.sqrt(D))).astype(jnp.bfloat16)


def shard_levels(rng, shape, shards, least, largest):
    gain = 1.0
    for dim, blocks in shards:
        draws = jax.random.uniform(jax.random.fold_in(jax.random.fold_in(rng, 6), dim), (blocks,), jnp.float32, least / len(shards), largest / len(shards))
        gain = gain * jnp.repeat(jnp.exp(draws), shape[dim] // blocks).reshape((-1,) + (1,) * (len(shape) - 1 - dim))
    return gain


def routed_block(own_key, own, number, rows, amount, top, limit, skew):
    order = jax.random.permutation(own_key, amount)
    heavy_load, ordinary = portions_of(amount, rows * top, limit, skew, True), portions_of(amount, rows * top, limit, skew, False)
    places = jnp.arange(amount)

    def named(tallies, rotation):
        used = int((tallies > 0).sum())
        fixed = max(1, used // 4)
        shifted = fixed + (places - fixed + rotation * (used - fixed)) % max(1, amount - fixed)
        return jnp.zeros((amount,), jnp.int32).at[order[jnp.where(places < fixed, places, shifted)]].set(jnp.asarray(tallies, jnp.int32))

    tallies = jnp.where(number % 4 == 0, named(heavy_load, number // 4), named(ordinary, number - number // 4 - 1))
    mixed = jax.random.permutation(jax.random.fold_in(own, 3), amount)
    giver, sink = mixed[0:amount // 2 * 2:2], mixed[1:amount // 2 * 2:2]
    room = jnp.minimum(tallies[giver] - 1, limit - tallies[sink]) // 2
    room = jnp.where((giver == order[0]) | (sink == order[0]) | (tallies[sink] == 0), 0, jnp.maximum(room, 0))
    shifted = jax.random.randint(jax.random.fold_in(own, 4), (amount // 2,), 0, 1 << 20) % (room + 1)
    tallies = tallies.at[giver].add(-shifted).at[sink].add(shifted)
    labels = jnp.searchsorted(jnp.cumsum(tallies), jnp.arange(rows * top), side="right").astype(jnp.int32)
    table = labels.reshape(top, rows).T
    table = table[jax.random.permutation(jax.random.fold_in(own, 1), rows)]
    rotation = jax.random.randint(jax.random.fold_in(own, 2), (rows, 1), 0, top)
    return jnp.take_along_axis(table, (jnp.arange(top)[None, :] + rotation) % top, axis=1)


def portions_of(count, total, most, skew, full):
    loads = [(1 << 20) // math.isqrt(grade ** skew) + 1 for grade in range(1, count + 1)]
    largest = most if full else min(most, max(-(-total // count), total * loads[0] // sum(loads)))
    least = 1 if total - largest >= count - 1 else 0
    counts, surplus = [largest] + [least] * (count - 1), total - largest - least * (count - 1)
    while surplus > 0:
        candidates = [i for i in range(1, count) if counts[i] < largest] or [i for i in range(1, count) if counts[i] < most]
        mass, remaining = sum([loads[i] for i in candidates]), surplus
        for i in candidates:
            more = min(most - counts[i], max(1, remaining * loads[i] // mass), surplus)
            counts[i] = counts[i] + more
            surplus = surplus - more
    return np.array(counts)


def bell_draw(key, shape, scale, most, pieces=(), kind=jnp.bfloat16):
    result = jax.random.normal(key, shape, jnp.float32) * scale
    if len(pieces) > 0:
        result = shard_levels(key, shape, pieces, -0.22, 0.18) * result
    return jnp.clip(result, min=-most, max=most).astype(kind)


def setup_inputs(seed: int = 0) -> dict:
    key_list = jax.random.split(jax.random.key(seed), 8)
    tokens = bell_draw(key_list[0], (TOKENS, D), 1.0, 6.0, ((0, 8),))
    expert_ids_keys = jax.random.split(jax.random.fold_in(key_list[1], 1), TOKENS // TOK_GROUP)
    expert_ids_turns = jax.random.permutation(jax.random.fold_in(key_list[1], 3), TOKENS // TOK_GROUP)
    expert_ids = jax.vmap(lambda own, number: routed_block(jax.random.fold_in(key_list[1], 2), own, number, TOK_GROUP, EXPERTS, TOP_K, CAP, 1))(expert_ids_keys, expert_ids_turns).reshape((TOKENS, TOP_K))
    route_weight = jnp.clip(0.1 + 0.9 * jax.random.uniform(key_list[2], (TOKENS, TOP_K), jnp.float32) ** shard_levels(key_list[2], (TOKENS, TOP_K), ((0, 8),), -0.2, 0.2), 0.1, 1.0)
    norm_gain = jnp.clip(1.0 + 0.18 * jax.random.normal(key_list[3], (D,), jnp.float32), 0.1, 1.9)
    expert_gate = draw_expert_gate(jax.random.fold_in(key_list[7], 71), 0)
    expert_up = draw_expert_up(jax.random.fold_in(key_list[7], 71), 0)
    expert_down = bell_draw(key_list[6], (EXPERTS, FF, D), (16 * FF) ** -0.5, 0.03125, ((0, 8), (1, 4)))
    return dict(tokens=tokens, expert_ids=expert_ids, route_weight=route_weight, norm_gain=norm_gain, expert_gate=expert_gate, expert_up=expert_up, expert_down=expert_down)


NORM_EPS = 1e-06
CLAMP_LIMIT = 7.0
SWISH_SCALE = 1.702

def normalize(tokens, norm_gain):
    values = tokens.astype(jnp.float32)
    scaled = values * lax.rsqrt(lax.optimization_barrier(jnp.mean(values * values, axis=-1, keepdims=True)) + NORM_EPS)
    return (scaled * norm_gain).astype(jnp.bfloat16)

def activate(gate_sum, up_sum):
    gate_cut = jnp.minimum(gate_sum, CLAMP_LIMIT)
    up_cut = jnp.clip(up_sum, -CLAMP_LIMIT, CLAMP_LIMIT)
    return ((up_cut + 1.0) * gate_cut * jax.nn.sigmoid(SWISH_SCALE * gate_cut)).astype(jnp.bfloat16)

def reference(tokens, expert_ids, route_weight, norm_gain, expert_gate, expert_up, expert_down):
    normed = normalize(tokens, norm_gain)
    flat_ids = expert_ids.reshape(N_EP, TOK_GROUP * TOP_K)
    onehot = (flat_ids[:, :, None] == jnp.arange(EXPERTS, dtype=jnp.int32)[None, None, :]).astype(jnp.int32)
    slot_index = lax.optimization_barrier(jnp.sum(jnp.cumsum(onehot, axis=1) * onehot, axis=2)) - 1
    block_index = jnp.arange(N_EP, dtype=jnp.int32)[:, None]
    token_index = block_index * TOK_GROUP + jnp.arange(TOK_GROUP * TOP_K, dtype=jnp.int32)[None, :] // TOP_K
    position = (block_index * CAP + slot_index).astype(jnp.int32)
    row_table = jnp.full((EXPERTS, N_EP * CAP), TOKENS, jnp.int32).at[flat_ids, position].set(token_index.astype(jnp.int32))
    padded = jnp.concatenate([normed, jnp.zeros((1, D), jnp.bfloat16)], axis=0)
    quarter = FF // N_TP

    def one_expert(operands):
        rows_index, gate_w, up_w, down_w = operands
        picked = padded[rows_index]
        gate_sum = jnp.dot(picked, gate_w, preferred_element_type=jnp.float32)
        up_sum = jnp.dot(picked, up_w, preferred_element_type=jnp.float32)
        activated = activate(gate_sum, up_sum)
        total_sum = jnp.zeros((picked.shape[0], D), jnp.float32)
        for shard_number in range(N_TP):
            lower = shard_number * quarter
            partial_value = jnp.dot(activated[:, lower:lower + quarter], down_w[lower:lower + quarter], preferred_element_type=jnp.float32)
            rounded = lax.optimization_barrier(partial_value.astype(jnp.bfloat16))
            total_sum = total_sum + rounded.astype(jnp.float32)
        return total_sum.astype(jnp.bfloat16)
    outputs = lax.map(one_expert, (row_table, expert_gate, expert_up, expert_down))
    flat_out = outputs.reshape(EXPERTS * N_EP * CAP, D)
    out_index = (flat_ids * (N_EP * CAP) + position).reshape(-1)
    chosen = flat_out[out_index].reshape(TOKENS, TOP_K, D).astype(jnp.float32)
    combined = lax.optimization_barrier(jnp.sum(chosen * route_weight[:, :, None], axis=1))
    return combined.astype(jnp.bfloat16)
```

```python
import functools

import jax
import jax.numpy as jnp
from jax import lax
from jax.experimental import pallas as pl
from jax.experimental.pallas import tpu as pltpu
from jax.sharding import PartitionSpec as P

NORM_EPS = 1e-06
CLAMP_LIMIT = 7.0
SWISH_SCALE = 1.702
MESH = pl.DeviceIdType.MESH
VISITS = (0, 2, 7, 6, 1, 4, 3, 5)


def activate(gate_sum, up_sum):
    gate_cut = jnp.minimum(gate_sum, CLAMP_LIMIT)
    up_cut = jnp.clip(up_sum, -CLAMP_LIMIT, CLAMP_LIMIT)
    return ((up_cut + 1.0) * gate_cut * jax.nn.sigmoid(SWISH_SCALE * gate_cut)).astype(jnp.bfloat16)


def expert_kernel(
    groups,
    tokens,
    ids,
    route,
    gain,
    gate_hbm,
    up_hbm,
    down_hbm,
    out,
    gate_w,
    up_w,
    down_w,
    normed_own,
    normed_cross,
    before,
    send,
    send_cross,
    back,
    high,
    low,
    total_out,
    rows,
    part,
    pair_in,
    cross_out,
    cross_in,
    result,
    w_sem,
    disp_send,
    disp_recv,
    cross_send,
    cross_recv,
    core_send,
    core_recv,
    fwd_send,
    fwd_recv,
    pair_send,
    pair_recv,
    sum_send,
    sum_recv,
    ret_send,
    ret_recv,
):
    me = lax.axis_index("ep")
    tp = lax.axis_index("tp")
    a, b = tp // 2, lax.rem(tp, 2)
    cross = 2 * (1 - a) + b
    core = 2 * a + 1 - b
    capacity, quarter = send.shape[1:]
    tok_count = tokens.shape[0]
    half = groups // 2

    weights = [
        pltpu.make_async_copy(src, dst, w_sem.at[i])
        for i, (src, dst) in enumerate(((gate_hbm, gate_w), (up_hbm, up_w), (down_hbm, down_w)))
    ]

    def remote(src, dst, send_sem, recv_sem, ep_index, tp_index):
        return pltpu.make_async_remote_copy(
            src_ref=src,
            dst_ref=dst,
            send_sem=send_sem,
            recv_sem=recv_sem,
            device_id=(ep_index, tp_index),
            device_id_type=MESH,
        )

    def partner(k):
        total, bit = 0, 1
        while bit < groups:
            total += bit * lax.rem(me // bit + k // bit, 2)
            bit *= 2
        return total

    def order(i):
        turn = lax.rem(i, len(VISITS))
        first = sum(place * (turn == n).astype(jnp.int32) for n, place in enumerate(VISITS))
        return first * (groups // len(VISITS)) + i // len(VISITS)

    def dispatch(k):
        dst = partner(k)
        return remote(send.at[k], rows.at[k, tp], disp_send.at[k], disp_recv.at[k], dst, tp)

    def dispatch_cross(k):
        dst = partner(k)
        return remote(
            send_cross.at[k],
            rows.at[k, cross],
            cross_send.at[k],
            cross_recv.at[k],
            dst,
            tp,
        )

    def to_cross(k):
        return remote(rows.at[k, tp], rows.at[k, tp], cross_send.at[k], cross_recv.at[k], me, cross)

    def to_core(k):
        return remote(rows.at[k, tp], rows.at[k, tp], core_send.at[k], core_recv.at[k], me, core)

    def forward(k):
        return remote(rows.at[k, cross], rows.at[k, cross], fwd_send.at[k], fwd_recv.at[k], me, core)

    def pair(k):
        return remote(part.at[k, 1 - b], pair_in.at[k], pair_send.at[k], pair_recv.at[k], me, core)

    def cross_sum(k):
        return remote(cross_out.at[k], cross_in.at[k], sum_send.at[k], sum_recv.at[k], me, cross)

    def give_back(k):
        return remote(result.at[k], back.at[k], ret_send.at[k], ret_recv.at[k], partner(k), tp)

    for copy in weights:
        copy.start()

    barrier = pltpu.get_barrier_semaphore()

    def greet(k, carry):
        pl.semaphore_signal(
            barrier, inc=1, device_id=(lax.rem(me + k, groups), tp), device_id_type=MESH
        )
        return carry

    lax.fori_loop(1, groups, greet, 0)
    pl.semaphore_signal(barrier, inc=1, device_id=(me, cross), device_id_type=MESH)
    pl.semaphore_signal(barrier, inc=1, device_id=(me, core), device_id_type=MESH)

    values = tokens[...].astype(jnp.float32)
    scale = lax.rsqrt(jnp.mean(values * values, axis=-1, keepdims=True) + NORM_EPS)

    def normed(index):
        span = pl.ds(pl.multiple_of(index * quarter, quarter), quarter)
        return (tokens[:, span].astype(jnp.float32) * scale * gain[:, span]).astype(jnp.bfloat16)

    normed_own[...] = normed(tp)
    normed_cross[...] = normed(cross)
    earlier = lax.broadcasted_iota(jnp.int32, (tok_count, tok_count), 0)
    later = lax.broadcasted_iota(jnp.int32, (tok_count, tok_count), 1)
    before[...] = jnp.where(earlier < later, 1.0, 0.0).astype(jnp.bfloat16)

    def select(k):
        expert = partner(k)
        hits = ids[...] == expert
        named = jnp.sum(jnp.where(hits, 1.0, 0.0), axis=0, keepdims=True)
        weight = jnp.sum(jnp.where(hits, route[...], 0.0), axis=0, keepdims=True)
        count = jnp.dot(
            jnp.broadcast_to(named, (8, tok_count)).astype(jnp.bfloat16),
            before[...],
            preferred_element_type=jnp.float32,
        )[0:1]
        slot = jnp.where(named > 0.0, count.astype(jnp.int32), -1)
        place = lax.broadcasted_iota(jnp.int32, (capacity, tok_count), 0)
        chosen = place == slot
        mix = jnp.where(chosen, weight, 0.0)
        mix_high = mix.astype(jnp.bfloat16)
        high[k] = mix_high
        low[k] = (mix - mix_high.astype(jnp.float32)).astype(jnp.bfloat16)
        return jnp.where(chosen, 1.0, 0.0).astype(jnp.bfloat16)

    def pick(chosen, source):
        return jnp.dot(chosen, source[...], preferred_element_type=jnp.float32).astype(jnp.bfloat16)

    chosen = select(0)
    rows[0, tp] = pick(chosen, normed_own)
    rows[0, cross] = pick(chosen, normed_cross)
    pl.semaphore_wait(barrier, groups + 1)

    def launch(i, carry):
        k = order(i)
        chosen = select(k)
        send[k] = pick(chosen, normed_own)
        dispatch(k).start()

        @pl.when(k < half)
        def _():
            send_cross[k] = pick(chosen, normed_cross)
            dispatch_cross(k).start()

        return carry

    lax.fori_loop(1, groups, launch, 0)
    for copy in weights:
        copy.wait()

    def step(i, carry):
        @pl.when((i >= 3) & (i < groups + 3))
        def _():
            k = order(i - 3)
            pair(k).wait_recv()
            total = part[k, b, 1 - a].astype(jnp.float32) + pair_in[k, 1 - a].astype(jnp.float32)
            cross_out[k] = total.astype(jnp.bfloat16)
            cross_sum(k).start()

        @pl.when((i >= 2) & (i < groups + 2))
        def _():
            k = order(i - 2)
            to_core(k).wait_recv()
            forward(k).wait_recv()
            block = jnp.concatenate([rows[k, j] for j in range(4)], axis=1)
            gate_sum = jnp.dot(block, gate_w[...], preferred_element_type=jnp.float32)
            up_sum = jnp.dot(block, up_w[...], preferred_element_type=jnp.float32)
            activated = activate(gate_sum, up_sum)
            for j in range(4):
                part[k, j % 2, j // 2] = jnp.dot(
                    activated,
                    down_w[:, j * quarter : (j + 1) * quarter],
                    preferred_element_type=jnp.float32,
                ).astype(jnp.bfloat16)
            pair(k).start()

        @pl.when(i >= 4)
        def _():
            k = order(i - 4)
            cross_sum(k).wait_recv()
            total = part[k, b, a].astype(jnp.float32) + pair_in[k, a].astype(jnp.float32)
            total = (total + cross_in[k].astype(jnp.float32)).astype(jnp.bfloat16)

            @pl.when(k == 0)
            def _():
                back[0] = total

            @pl.when(k > 0)
            def _():
                result[k] = total
                give_back(k).start()

        @pl.when(i < groups)
        def _():
            k = order(i)

            @pl.when(k > 0)
            def _():
                dispatch(k).wait_recv()

            @pl.when(k >= half)
            def _():
                to_cross(k).start()

            to_core(k).start()

        @pl.when((i >= 1) & (i < groups + 1))
        def _():
            k = order(i - 1)

            @pl.when(k > 0)
            def _():
                to_cross(k).wait_recv()

            forward(k).start()

        return carry

    lax.fori_loop(0, groups + 4, step, 0)

    total_out[...] = jnp.zeros_like(total_out)

    def finish(i, carry):
        k = order(i)

        @pl.when(k > 0)
        def _():
            give_back(k).wait_recv()

        for share in (high, low):
            total_out[...] += lax.dot_general(
                share[k], back[k], (((0,), (0,)), ((), ())), preferred_element_type=jnp.float32
            )
        return carry

    lax.fori_loop(0, groups, finish, 0)
    out[...] = total_out[...].astype(jnp.bfloat16)

    def drain(k, carry):
        to_core(k).wait_send()
        forward(k).wait_send()
        pair(k).wait_send()
        cross_sum(k).wait_send()

        @pl.when(k > 0)
        def _():
            to_cross(k).wait_send()
            dispatch(k).wait_send()
            give_back(k).wait_send()

        return carry

    lax.fori_loop(0, groups, drain, 0)


def shards(tokens, expert_ids, route_weight, norm_gain, expert_gate, expert_up, expert_down):
    groups = lax.axis_size("ep")
    tp_count = lax.axis_size("tp")
    experts = groups * expert_gate.shape[0]
    tok_count, model_width = tokens.shape
    top_count = expert_ids.shape[1]
    capacity = min(tok_count, 3 * tok_count * top_count // experts)
    quarter = model_width // tp_count
    bf16 = jnp.bfloat16
    slots = (groups, capacity, quarter)
    weights = (expert_gate[0], expert_up[0], expert_down[0])
    return pl.pallas_call(
        functools.partial(expert_kernel, groups),
        out_shape=jax.ShapeDtypeStruct((tok_count, quarter), bf16),
        in_specs=[pl.BlockSpec(memory_space=pltpu.VMEM)] * 4
        + [pl.BlockSpec(memory_space=pl.ANY)] * 3,
        out_specs=pl.BlockSpec(memory_space=pltpu.VMEM),
        scratch_shapes=[
            *[pltpu.VMEM(weight.shape, bf16) for weight in weights],
            pltpu.VMEM((tok_count, quarter), bf16),
            pltpu.VMEM((tok_count, quarter), bf16),
            pltpu.VMEM((tok_count, tok_count), bf16),
            pltpu.VMEM(slots, bf16),
            pltpu.VMEM((groups // 2, capacity, quarter), bf16),
            pltpu.VMEM(slots, bf16),
            pltpu.VMEM((groups, capacity, tok_count), bf16),
            pltpu.VMEM((groups, capacity, tok_count), bf16),
            pltpu.VMEM((tok_count, quarter), jnp.float32),
            pltpu.VMEM((groups, 4, capacity, quarter), bf16),
            pltpu.VMEM((groups, 2, 2, capacity, quarter), bf16),
            pltpu.VMEM((groups, 2, capacity, quarter), bf16),
            pltpu.VMEM(slots, bf16),
            pltpu.VMEM(slots, bf16),
            pltpu.VMEM(slots, bf16),
            pltpu.SemaphoreType.DMA((3,)),
            *[pltpu.SemaphoreType.DMA((groups,)) for _ in range(14)],
        ],
        compiler_params=pltpu.CompilerParams(
            collective_id=0, has_side_effects=True, vmem_limit_bytes=60 * 1024 * 1024
        ),
    )(tokens, expert_ids.T, route_weight.T, norm_gain[None, :], *weights)


def solution(mesh):
    return jax.shard_map(
        shards,
        mesh=mesh,
        in_specs=(
            P("ep", None),
            P("ep", None),
            P("ep", None),
            P(),
            P("ep", None, "tp"),
            P("ep", None, "tp"),
            P("ep", "tp", None),
        ),
        out_specs=P("ep", "tp"),
        check_vma=False,
    )
```

```python
import functools

import jax
import jax.numpy as jnp
from jax import lax
from jax.experimental import pallas as pl
from jax.experimental.pallas import tpu as pltpu
from jax.sharding import PartitionSpec as P

NORM_EPS = 1e-06
CLAMP_LIMIT = 7.0
SWISH_SCALE = 1.702
MESH = pl.DeviceIdType.MESH
STEPS = (
    "L30", "M0", "Y00", "A00", "L31", "F00", "G000", "G001", "L20", "M3",
    "Y30", "A30", "L11", "B01", "L21", "H001", "B00", "B30", "A31", "F01",
    "Y31", "G010", "X300", "M2", "A20", "Y20", "X301", "L10", "B31", "F30",
    "B20", "Y21", "A21", "X310", "M1", "A11", "X311", "Y11", "G300", "F31",
    "B21", "X210", "X200", "G311", "G310", "G301", "A10", "H300", "Y10", "X201",
    "G011", "H000", "X211", "F10", "H311", "F20", "F21", "G100", "H301", "B11",
    "H310", "B10", "G210", "S31", "G200", "F11", "H010", "S30", "G110", "G211",
    "G111", "H210", "H200", "G201", "H011", "H100", "G101", "H110", "S20", "H211",
    "J30", "H111", "S00", "S10", "H201", "H101", "S21", "J31", "J10", "S11",
    "S01", "J20", "J11", "J21",
)
PLANES = 1 + max(int(step[1]) for step in STEPS)
PARTS = 2


def activate(gate_sum, up_sum):
    gate_cut = jnp.minimum(gate_sum, CLAMP_LIMIT)
    up_cut = jnp.clip(up_sum, -CLAMP_LIMIT, CLAMP_LIMIT)
    return ((up_cut + 1.0) * gate_cut * jax.nn.sigmoid(SWISH_SCALE * gate_cut)).astype(jnp.bfloat16)


def plane_kernel(
    groups,
    tokens,
    ids,
    route,
    gain,
    gate_hbm,
    up_hbm,
    down_hbm,
    out,
    gate_w,
    up_w,
    down_w,
    before,
    meta,
    normed,
    dense,
    picker,
    high,
    low,
    rows,
    picked,
    part,
    pair_in,
    cross_out,
    cross_in,
    result,
    plane_in,
    total,
    sum_out,
    sum_in,
    w_sem,
    meta_send,
    meta_recv,
    dense_send,
    dense_recv,
    pick_send,
    pick_recv,
    core_send,
    core_recv,
    fwd_send,
    fwd_recv,
    pair_send,
    pair_recv,
    cross_send,
    cross_recv,
    near_send,
    near_recv,
    sum_send,
    sum_recv,
):
    me = lax.axis_index("ep")
    tp = lax.axis_index("tp")
    a, b = tp // 2, lax.rem(tp, 2)
    cross = 2 * (1 - a) + b
    core = 2 * a + 1 - b
    quarters = (tp, cross)
    slots, width = rows.shape[3:]
    quarter = PARTS * width
    tok_count = tokens.shape[0]
    f32, bf16 = jnp.float32, jnp.bfloat16

    def partner(k):
        total, bit = 0, 1
        while bit < groups:
            total += bit * lax.rem(me // bit + k // bit, 2)
            bit *= 2
        return total

    def remote(src, dst, send_sem, recv_sem, k, tp_index):
        return pltpu.make_async_remote_copy(
            src_ref=src,
            dst_ref=dst,
            send_sem=send_sem,
            recv_sem=recv_sem,
            device_id=(partner(k), tp_index),
            device_id_type=MESH,
        )

    def shares(d):
        return range(2 if d < PLANES // 2 else 1)

    def describe(d):
        return remote(meta.at[0], meta.at[d], meta_send.at[d], meta_recv.at[d], 2 * d, tp)

    def spread(d, q, h):
        return remote(
            normed.at[quarters[q], h],
            dense.at[d - 1, q, h],
            dense_send.at[d, q, h],
            dense_recv.at[d, q, h],
            2 * d,
            tp,
        )

    def neighbour(d, q, h):
        return remote(
            picked.at[d, q, h],
            rows.at[2 * d + 1, quarters[q], h],
            pick_send.at[d, q, h],
            pick_recv.at[d, q, h],
            1,
            tp,
        )

    def to_core(k, q, h):
        ref = rows.at[k, quarters[q], h]
        return remote(ref, ref, core_send.at[k, q, h], core_recv.at[k, q, h], 0, core)

    def to_cross(k, h):
        ref = rows.at[k, tp, h]
        return remote(ref, ref, fwd_send.at[k, h], fwd_recv.at[k, h], 0, cross)

    def pair(k, h):
        return remote(
            part.at[k, 1 - b, h], pair_in.at[k, h], pair_send.at[k, h], pair_recv.at[k, h], 0, core
        )

    def cross_sum(k, h):
        return remote(
            cross_out.at[k, h], cross_in.at[k, h], cross_send.at[k, h], cross_recv.at[k, h], 0, cross
        )

    def near_sum(d, h):
        return remote(
            result.at[2 * d + 1, h], plane_in.at[d, h], near_send.at[d, h], near_recv.at[d, h], 1, tp
        )

    def plane_sum(d, h):
        return remote(
            sum_out.at[d - 1, h], sum_in.at[d - 1, h], sum_send.at[d, h], sum_recv.at[d, h], 2 * d, tp
        )

    weights = [
        pltpu.make_async_copy(src, dst, w_sem.at[i])
        for i, (src, dst) in enumerate(((gate_hbm, gate_w), (up_hbm, up_w), (down_hbm, down_w)))
    ]
    for copy in weights:
        copy.start()

    barrier = pltpu.get_barrier_semaphore()
    peers = [(partner(2 * d), tp) for d in range(1, PLANES)]
    peers += [(partner(1), tp), (me, cross), (me, core)]
    for peer in peers:
        pl.semaphore_signal(barrier, inc=1, device_id=peer, device_id_type=MESH)

    values = tokens[...].astype(f32)
    scale = lax.rsqrt(jnp.mean(values * values, axis=-1, keepdims=True) + NORM_EPS)
    for j in range(4):
        for h in range(PARTS):
            span = slice(j * quarter + h * width, j * quarter + (h + 1) * width)
            normed[j, h] = (tokens[:, span].astype(f32) * scale * gain[:, span]).astype(bf16)
    meta[0, 0:2] = ids[...].astype(f32)
    meta[0, 2:4] = route[...]
    pl.semaphore_wait(barrier, len(peers))
    for d in range(1, PLANES):
        describe(d).start()

    def L(d, h):
        for q in shares(d):
            spread(d, q, h).start()

    def M(d):
        if d:
            describe(d).wait_recv()
        else:
            earlier = lax.broadcasted_iota(jnp.int32, (tok_count, tok_count), 0)
            later = lax.broadcasted_iota(jnp.int32, (tok_count, tok_count), 1)
            before[...] = jnp.where(earlier < later, 1.0, 0.0).astype(bf16)
        for side in range(2):
            hits = meta[d, 0:2] == partner(side).astype(f32)
            named = jnp.sum(jnp.where(hits, 1.0, 0.0), axis=0, keepdims=True)
            weight = jnp.sum(jnp.where(hits, meta[d, 2:4], 0.0), axis=0, keepdims=True)
            count = jnp.dot(
                jnp.broadcast_to(named, (8, tok_count)).astype(bf16),
                before[...],
                preferred_element_type=f32,
            )[0:1]
            slot = jnp.where(named > 0.0, count.astype(jnp.int32), -1)
            place = lax.broadcasted_iota(jnp.int32, (slots, tok_count), 0)
            chosen = place == slot
            mix = jnp.where(chosen, weight, 0.0)
            mix_high = mix.astype(bf16)
            high[d, side] = mix_high
            low[d, side] = (mix - mix_high.astype(f32)).astype(bf16)
            picker[d, side] = jnp.where(chosen, 1.0, 0.0).astype(bf16)

    def block(d, q, h):
        return dense[d - 1, q, h] if d else normed[quarters[q], h]

    def pick(d, side, source):
        return jnp.dot(picker[d, side], source, preferred_element_type=f32).astype(bf16)

    arrived = set()

    def arrive(d, h):
        if d and (d, h) not in arrived:
            arrived.add((d, h))
            for q in shares(d):
                spread(d, q, h).wait_recv()

    def A(d, h):
        if d == 0:
            for j in range(4):
                for n in range(PARTS):
                    rows[0, j, n] = pick(0, 0, normed[j, n])
            return
        arrive(d, h)
        for q in shares(d):
            rows[2 * d, quarters[q], h] = pick(d, 0, block(d, q, h))
            to_core(2 * d, q, h).start()
        if len(shares(d)) == 1:
            to_cross(2 * d, h).start()

    def Y(d, h):
        arrive(d, h)
        for n in range(PARTS) if d == 0 else (h,):
            for q in shares(d):
                picked[d, q, n] = pick(d, 1, block(d, q, n))
                neighbour(d, q, n).start()

    def B(d, h):
        k = 2 * d + 1
        for q in shares(d):
            neighbour(d, q, h).wait_recv()
            to_core(k, q, h).start()
        if len(shares(d)) == 1:
            to_cross(k, h).start()

    def X(d, side, h):
        k = 2 * d + side
        to_cross(k, h).wait_recv()
        to_core(k, 1, h).start()

    def F(d, side):
        k = 2 * d + side
        if (d, side) == FIRST:
            for copy in weights:
                copy.wait()
        if k:
            for q in range(2):
                for h in range(PARTS):
                    to_core(k, q, h).wait_recv()
        whole = jnp.concatenate([rows[k, j, h] for j in range(4) for h in range(PARTS)], axis=1)
        gate_sum = jnp.dot(whole, gate_w[...], preferred_element_type=f32)
        up_sum = jnp.dot(whole, up_w[...], preferred_element_type=f32)
        activated = activate(gate_sum, up_sum)
        for j in range(4):
            piece = jnp.dot(
                activated, down_w[:, j * quarter : (j + 1) * quarter], preferred_element_type=f32
            ).astype(bf16)
            for h in range(PARTS):
                part[k, j % 2, h, j // 2] = piece[:, h * width : (h + 1) * width]
        for h in range(PARTS):
            pair(k, h).start()

    def G(d, side, h):
        k = 2 * d + side
        pair(k, h).wait_recv()
        both = part[k, b, h, 1 - a].astype(f32) + pair_in[k, h, 1 - a].astype(f32)
        cross_out[k, h] = both.astype(bf16)
        cross_sum(k, h).start()

    def H(d, side, h):
        k = 2 * d + side
        cross_sum(k, h).wait_recv()
        both = part[k, b, h, a].astype(f32) + pair_in[k, h, a].astype(f32)
        result[k, h] = (both + cross_in[k, h].astype(f32)).astype(bf16)
        if side:
            near_sum(d, h).start()

    def S(d, h):
        near_sum(d, h).wait_recv()
        mixed = 0.0
        for side, value in ((0, result[2 * d, h]), (1, plane_in[d, h])):
            for share in (high, low):
                mixed += lax.dot_general(
                    share[d, side], value, (((0,), (0,)), ((), ())), preferred_element_type=f32
                )
        if d:
            sum_out[d - 1, h] = mixed.astype(bf16)
            plane_sum(d, h).start()
        else:
            total[h] = mixed

    def J(d, h):
        plane_sum(d, h).wait_recv()

    stages = dict(L=L, M=M, A=A, Y=Y, B=B, X=X, F=F, G=G, H=H, S=S, J=J)
    for step in STEPS:
        stages[step[0]](*(int(n) for n in step[1:]))

    for h in range(PARTS):
        mixed = total[h]
        for d in range(1, PLANES):
            mixed += sum_in[d - 1, h].astype(f32)
        out[:, h * width : (h + 1) * width] = mixed.astype(bf16)

    for d in range(PLANES):
        if d:
            describe(d).wait_send()
        for h in range(PARTS):
            for q in shares(d):
                neighbour(d, q, h).wait_send()
                if d:
                    spread(d, q, h).wait_send()
            near_sum(d, h).wait_send()
            if d:
                plane_sum(d, h).wait_send()
    for k in range(groups):
        for h in range(PARTS):
            pair(k, h).wait_send()
            cross_sum(k, h).wait_send()
            if k:
                for q in range(2):
                    to_core(k, q, h).wait_send()
            if k >= PLANES:
                to_cross(k, h).wait_send()


FIRST = next((int(step[1]), int(step[2])) for step in STEPS if step[0] == "F")


def plane_call(groups, capacity, operands):
    tokens, weights = operands[0], operands[4:]
    tok_count, model_width = tokens.shape
    quarter = model_width // 4
    width = quarter // PARTS
    bf16, f32 = jnp.bfloat16, jnp.float32
    compact = (PARTS, capacity, width)
    full = (PARTS, tok_count, width)
    dma = pltpu.SemaphoreType.DMA
    return pl.pallas_call(
        functools.partial(plane_kernel, groups),
        out_shape=jax.ShapeDtypeStruct((tok_count, quarter), bf16),
        in_specs=[pl.BlockSpec(memory_space=pltpu.VMEM)] * 4
        + [pl.BlockSpec(memory_space=pl.ANY)] * 3,
        out_specs=pl.BlockSpec(memory_space=pltpu.VMEM),
        scratch_shapes=[
            *[pltpu.VMEM(weight.shape, bf16) for weight in weights],
            pltpu.VMEM((tok_count, tok_count), bf16),
            pltpu.VMEM((PLANES, 8, tok_count), f32),
            pltpu.VMEM((4, *full), bf16),
            pltpu.VMEM((PLANES - 1, 2, *full), bf16),
            *[pltpu.VMEM((PLANES, 2, capacity, tok_count), bf16)] * 3,
            pltpu.VMEM((groups, 4, *compact), bf16),
            pltpu.VMEM((PLANES, 2, *compact), bf16),
            pltpu.VMEM((groups, 2, PARTS, 2, capacity, width), bf16),
            pltpu.VMEM((groups, PARTS, 2, capacity, width), bf16),
            *[pltpu.VMEM((groups, *compact), bf16)] * 3,
            pltpu.VMEM((PLANES, *compact), bf16),
            pltpu.VMEM(full, f32),
            *[pltpu.VMEM((PLANES - 1, *full), bf16)] * 2,
            dma((3,)),
            *[dma((PLANES,))] * 2,
            *[dma((PLANES, 2, PARTS))] * 4,
            *[dma((groups, 2, PARTS))] * 2,
            *[dma((groups, PARTS))] * 6,
            *[dma((PLANES, PARTS))] * 4,
        ],
        compiler_params=pltpu.CompilerParams(
            collective_id=0, has_side_effects=True, vmem_limit_bytes=60 * 1024 * 1024
        ),
    )(*operands)


def expert_kernel(
    groups,
    tokens,
    ids,
    route,
    gain,
    gate_hbm,
    up_hbm,
    down_hbm,
    out,
    gate_w,
    up_w,
    down_w,
    normed_own,
    normed_cross,
    before,
    send,
    send_cross,
    back,
    high,
    low,
    total_out,
    rows,
    part,
    pair_in,
    cross_out,
    cross_in,
    result,
    w_sem,
    disp_send,
    disp_recv,
    cross_send,
    cross_recv,
    core_send,
    core_recv,
    fwd_send,
    fwd_recv,
    pair_send,
    pair_recv,
    sum_send,
    sum_recv,
    ret_send,
    ret_recv,
):
    me = lax.axis_index("ep")
    tp = lax.axis_index("tp")
    a, b = tp // 2, lax.rem(tp, 2)
    cross = 2 * (1 - a) + b
    core = 2 * a + 1 - b
    capacity, quarter = send.shape[1:]
    tok_count = tokens.shape[0]
    half = groups // 2

    weights = [
        pltpu.make_async_copy(src, dst, w_sem.at[i])
        for i, (src, dst) in enumerate(((gate_hbm, gate_w), (up_hbm, up_w), (down_hbm, down_w)))
    ]

    def remote(src, dst, send_sem, recv_sem, ep_index, tp_index):
        return pltpu.make_async_remote_copy(
            src_ref=src,
            dst_ref=dst,
            send_sem=send_sem,
            recv_sem=recv_sem,
            device_id=(ep_index, tp_index),
            device_id_type=MESH,
        )

    def partner(k):
        total, bit = 0, 1
        while bit < groups:
            total += bit * lax.rem(me // bit + k // bit, 2)
            bit *= 2
        return total

    def order(i):
        i = i + (i // (groups - 2)) * (1 - 2 * lax.rem(i, 2))
        return i // 2 + half * lax.rem(i, 2)

    def dispatch(k):
        dst = partner(k)
        return remote(send.at[k], rows.at[k, tp], disp_send.at[k], disp_recv.at[k], dst, tp)

    def dispatch_cross(k):
        dst = partner(k)
        return remote(
            send_cross.at[k],
            rows.at[k, cross],
            cross_send.at[k],
            cross_recv.at[k],
            dst,
            tp,
        )

    def to_cross(k):
        return remote(rows.at[k, tp], rows.at[k, tp], cross_send.at[k], cross_recv.at[k], me, cross)

    def to_core(k):
        return remote(rows.at[k, tp], rows.at[k, tp], core_send.at[k], core_recv.at[k], me, core)

    def forward(k):
        return remote(rows.at[k, cross], rows.at[k, cross], fwd_send.at[k], fwd_recv.at[k], me, core)

    def pair(k):
        return remote(part.at[k, 1 - b], pair_in.at[k], pair_send.at[k], pair_recv.at[k], me, core)

    def cross_sum(k):
        return remote(cross_out.at[k], cross_in.at[k], sum_send.at[k], sum_recv.at[k], me, cross)

    def give_back(k):
        return remote(result.at[k], back.at[k], ret_send.at[k], ret_recv.at[k], partner(k), tp)

    for copy in weights:
        copy.start()

    barrier = pltpu.get_barrier_semaphore()

    def greet(k, carry):
        pl.semaphore_signal(
            barrier, inc=1, device_id=(lax.rem(me + k, groups), tp), device_id_type=MESH
        )
        return carry

    lax.fori_loop(1, groups, greet, 0)
    pl.semaphore_signal(barrier, inc=1, device_id=(me, cross), device_id_type=MESH)
    pl.semaphore_signal(barrier, inc=1, device_id=(me, core), device_id_type=MESH)

    values = tokens[...].astype(jnp.float32)
    scale = lax.rsqrt(jnp.mean(values * values, axis=-1, keepdims=True) + NORM_EPS)

    def normed(index):
        span = pl.ds(pl.multiple_of(index * quarter, quarter), quarter)
        return (tokens[:, span].astype(jnp.float32) * scale * gain[:, span]).astype(jnp.bfloat16)

    normed_own[...] = normed(tp)
    normed_cross[...] = normed(cross)
    earlier = lax.broadcasted_iota(jnp.int32, (tok_count, tok_count), 0)
    later = lax.broadcasted_iota(jnp.int32, (tok_count, tok_count), 1)
    before[...] = jnp.where(earlier < later, 1.0, 0.0).astype(jnp.bfloat16)

    def select(k):
        expert = partner(k)
        hits = ids[...] == expert
        named = jnp.sum(jnp.where(hits, 1.0, 0.0), axis=0, keepdims=True)
        weight = jnp.sum(jnp.where(hits, route[...], 0.0), axis=0, keepdims=True)
        count = jnp.dot(
            jnp.broadcast_to(named, (8, tok_count)).astype(jnp.bfloat16),
            before[...],
            preferred_element_type=jnp.float32,
        )[0:1]
        slot = jnp.where(named > 0.0, count.astype(jnp.int32), -1)
        place = lax.broadcasted_iota(jnp.int32, (capacity, tok_count), 0)
        chosen = place == slot
        mix = jnp.where(chosen, weight, 0.0)
        mix_high = mix.astype(jnp.bfloat16)
        high[k] = mix_high
        low[k] = (mix - mix_high.astype(jnp.float32)).astype(jnp.bfloat16)
        return jnp.where(chosen, 1.0, 0.0).astype(jnp.bfloat16)

    def pick(chosen, source):
        return jnp.dot(chosen, source[...], preferred_element_type=jnp.float32).astype(jnp.bfloat16)

    chosen = select(0)
    rows[0, tp] = pick(chosen, normed_own)
    rows[0, cross] = pick(chosen, normed_cross)
    pl.semaphore_wait(barrier, groups + 1)

    def launch(i, carry):
        k = order(i)
        chosen = select(k)
        send[k] = pick(chosen, normed_own)
        dispatch(k).start()

        @pl.when(k < half)
        def _():
            send_cross[k] = pick(chosen, normed_cross)
            dispatch_cross(k).start()

        return carry

    lax.fori_loop(1, groups, launch, 0)
    for copy in weights:
        copy.wait()

    def step(i, carry):
        @pl.when(i >= 4)
        def _():
            k = order(i - 4)
            cross_sum(k).wait_recv()
            total = part[k, b, a].astype(jnp.float32) + pair_in[k, a].astype(jnp.float32)
            total = (total + cross_in[k].astype(jnp.float32)).astype(jnp.bfloat16)

            @pl.when(k == 0)
            def _():
                back[0] = total

            @pl.when(k > 0)
            def _():
                result[k] = total
                give_back(k).start()

        @pl.when((i >= 3) & (i < groups + 3))
        def _():
            k = order(i - 3)
            pair(k).wait_recv()
            total = part[k, b, 1 - a].astype(jnp.float32) + pair_in[k, 1 - a].astype(jnp.float32)
            cross_out[k] = total.astype(jnp.bfloat16)
            cross_sum(k).start()

        @pl.when((i >= 2) & (i < groups + 2))
        def _():
            k = order(i - 2)
            to_core(k).wait_recv()
            forward(k).wait_recv()
            block = jnp.concatenate([rows[k, j] for j in range(4)], axis=1)
            gate_sum = jnp.dot(block, gate_w[...], preferred_element_type=jnp.float32)
            up_sum = jnp.dot(block, up_w[...], preferred_element_type=jnp.float32)
            activated = activate(gate_sum, up_sum)
            for j in range(4):
                part[k, j % 2, j // 2] = jnp.dot(
                    activated,
                    down_w[:, j * quarter : (j + 1) * quarter],
                    preferred_element_type=jnp.float32,
                ).astype(jnp.bfloat16)
            pair(k).start()

        @pl.when((i >= 1) & (i < groups + 1))
        def _():
            k = order(i - 1)

            @pl.when(k > 0)
            def _():
                to_cross(k).wait_recv()

            forward(k).start()

        @pl.when(i < groups)
        def _():
            k = order(i)

            @pl.when(k > 0)
            def _():
                dispatch(k).wait_recv()

            @pl.when(k >= half)
            def _():
                to_cross(k).start()

            to_core(k).start()

        return carry

    lax.fori_loop(0, groups + 4, step, 0)

    total_out[...] = jnp.zeros_like(total_out)

    def finish(i, carry):
        k = order(i)

        @pl.when(k > 0)
        def _():
            give_back(k).wait_recv()

        for share in (high, low):
            total_out[...] += lax.dot_general(
                share[k], back[k], (((0,), (0,)), ((), ())), preferred_element_type=jnp.float32
            )
        return carry

    lax.fori_loop(0, groups, finish, 0)
    out[...] = total_out[...].astype(jnp.bfloat16)

    def drain(k, carry):
        to_core(k).wait_send()
        forward(k).wait_send()
        pair(k).wait_send()
        cross_sum(k).wait_send()

        @pl.when(k > 0)
        def _():
            to_cross(k).wait_send()
            dispatch(k).wait_send()
            give_back(k).wait_send()

        return carry

    lax.fori_loop(0, groups, drain, 0)


def shards(tokens, expert_ids, route_weight, norm_gain, expert_gate, expert_up, expert_down):
    groups = lax.axis_size("ep")
    tp_count = lax.axis_size("tp")
    experts = groups * expert_gate.shape[0]
    tok_count, model_width = tokens.shape
    top_count = expert_ids.shape[1]
    capacity = min(tok_count, 3 * tok_count * top_count // experts)
    quarter = model_width // tp_count
    bf16 = jnp.bfloat16
    slots = (groups, capacity, quarter)
    weights = (expert_gate[0], expert_up[0], expert_down[0])
    operands = (tokens, expert_ids.T, route_weight.T, norm_gain[None, :], *weights)
    if groups == 2 * PLANES and 2 * capacity > tok_count:
        return plane_call(groups, capacity, operands)
    return pl.pallas_call(
        functools.partial(expert_kernel, groups),
        out_shape=jax.ShapeDtypeStruct((tok_count, quarter), bf16),
        in_specs=[pl.BlockSpec(memory_space=pltpu.VMEM)] * 4
        + [pl.BlockSpec(memory_space=pl.ANY)] * 3,
        out_specs=pl.BlockSpec(memory_space=pltpu.VMEM),
        scratch_shapes=[
            *[pltpu.VMEM(weight.shape, bf16) for weight in weights],
            pltpu.VMEM((tok_count, quarter), bf16),
            pltpu.VMEM((tok_count, quarter), bf16),
            pltpu.VMEM((tok_count, tok_count), bf16),
            pltpu.VMEM(slots, bf16),
            pltpu.VMEM((groups // 2, capacity, quarter), bf16),
            pltpu.VMEM(slots, bf16),
            pltpu.VMEM((groups, capacity, tok_count), bf16),
            pltpu.VMEM((groups, capacity, tok_count), bf16),
            pltpu.VMEM((tok_count, quarter), jnp.float32),
            pltpu.VMEM((groups, 4, capacity, quarter), bf16),
            pltpu.VMEM((groups, 2, 2, capacity, quarter), bf16),
            pltpu.VMEM((groups, 2, capacity, quarter), bf16),
            pltpu.VMEM(slots, bf16),
            pltpu.VMEM(slots, bf16),
            pltpu.VMEM(slots, bf16),
            pltpu.SemaphoreType.DMA((3,)),
            *[pltpu.SemaphoreType.DMA((groups,)) for _ in range(14)],
        ],
        compiler_params=pltpu.CompilerParams(
            collective_id=0, has_side_effects=True, vmem_limit_bytes=60 * 1024 * 1024
        ),
    )(*operands)


def solution(mesh):
    return jax.shard_map(
        shards,
        mesh=mesh,
        in_specs=(
            P("ep", None),
            P("ep", None),
            P("ep", None),
            P(),
            P("ep", None, "tp"),
            P("ep", None, "tp"),
            P("ep", "tp", None),
        ),
        out_specs=P("ep", "tp"),
        check_vma=False,
    )
```

```python
import functools

import jax
import jax.numpy as jnp
from jax import lax
from jax.experimental import pallas as pl
from jax.experimental.pallas import tpu as pltpu
from jax.sharding import PartitionSpec as P

NORM_EPS = 1e-06
CLAMP_LIMIT = 7.0
SWISH_SCALE = 1.702
MESH = pl.DeviceIdType.MESH
STEPS = (
    "L31", "L30", "L10", "M0", "Y00", "L21", "M3", "Y31", "B01", "B00",
    "L11", "A31", "B31", "A30", "Y30", "F01", "M1", "Y10", "L20", "G010",
    "B30", "X301", "M2", "Y21", "X311", "A21", "X300", "F30", "Y11", "G300",
    "X310", "B10", "A11", "B21", "F31", "G311", "A10", "Y20", "H300", "G310",
    "B11", "G301", "F10", "F11", "A20", "H311", "G100", "G110", "X211", "X201",
    "G111", "H310", "B20", "F21", "H301", "S31", "G210", "H110", "G211", "S30",
    "H010", "F20", "G200", "G101", "G201", "H210", "H100", "S10", "A00", "F00",
    "H111", "H200", "S20", "J31", "G011", "H211", "G000", "J30", "H101", "S11",
    "H201", "S21", "J10", "H011", "G001", "H001", "J20", "S01", "J11", "H000",
    "S00", "J21",
)
CARRIED = ((2, 2), (2, 2), (2, 1), (1, 1))
PLANES, PARTS = len(CARRIED), len(CARRIED[0])


def activate(gate_sum, up_sum):
    gate_cut = jnp.minimum(gate_sum, CLAMP_LIMIT)
    up_cut = jnp.clip(up_sum, -CLAMP_LIMIT, CLAMP_LIMIT)
    return ((up_cut + 1.0) * gate_cut * jax.nn.sigmoid(SWISH_SCALE * gate_cut)).astype(jnp.bfloat16)


def plane_kernel(
    groups,
    tokens,
    ids,
    route,
    gain,
    gate_hbm,
    up_hbm,
    down_hbm,
    out,
    gate_w,
    up_w,
    down_w,
    token_in,
    out_part,
    before,
    meta,
    normed,
    dense,
    picker,
    high,
    low,
    rows,
    picked,
    part,
    pair_in,
    cross_out,
    cross_in,
    result,
    plane_in,
    total,
    sum_out,
    sum_in,
    w_sem,
    io_sem,
    meta_send,
    meta_recv,
    dense_send,
    dense_recv,
    pick_send,
    pick_recv,
    core_send,
    core_recv,
    fwd_send,
    fwd_recv,
    pair_send,
    pair_recv,
    cross_send,
    cross_recv,
    near_send,
    near_recv,
    sum_send,
    sum_recv,
):
    me = lax.axis_index("ep")
    tp = lax.axis_index("tp")
    a, b = tp // 2, lax.rem(tp, 2)
    cross = 2 * (1 - a) + b
    core = 2 * a + 1 - b
    quarters = (tp, cross)
    slots, width = rows.shape[3:]
    quarter = PARTS * width
    tok_count = tokens.shape[0]
    f32, bf16 = jnp.float32, jnp.bfloat16
    fetch = pltpu.make_async_copy(tokens, token_in, io_sem.at[PARTS])
    fetch.start()

    def partner(k):
        total, bit = 0, 1
        while bit < groups:
            total += bit * lax.rem(me // bit + k // bit, 2)
            bit *= 2
        return total

    def remote(src, dst, send_sem, recv_sem, k, tp_index):
        return pltpu.make_async_remote_copy(
            src_ref=src,
            dst_ref=dst,
            send_sem=send_sem,
            recv_sem=recv_sem,
            device_id=(partner(k), tp_index),
            device_id_type=MESH,
        )

    def shares(d, h):
        return range(CARRIED[d][h])

    def describe(d):
        return remote(meta.at[0], meta.at[d], meta_send.at[d], meta_recv.at[d], 2 * d, tp)

    def spread(d, q, h):
        return remote(
            normed.at[quarters[q], h],
            dense.at[d - 1, q, h],
            dense_send.at[d, q, h],
            dense_recv.at[d, q, h],
            2 * d,
            tp,
        )

    def neighbour(d, q, h):
        return remote(
            picked.at[d, q, h],
            rows.at[2 * d + 1, quarters[q], h],
            pick_send.at[d, q, h],
            pick_recv.at[d, q, h],
            1,
            tp,
        )

    def to_core(k, q, h):
        ref = rows.at[k, quarters[q], h]
        return remote(ref, ref, core_send.at[k, q, h], core_recv.at[k, q, h], 0, core)

    def to_cross(k, h):
        ref = rows.at[k, tp, h]
        return remote(ref, ref, fwd_send.at[k, h], fwd_recv.at[k, h], 0, cross)

    def pair(k, h):
        return remote(
            part.at[k, 1 - b, h], pair_in.at[k, h], pair_send.at[k, h], pair_recv.at[k, h], 0, core
        )

    def cross_sum(k, h):
        return remote(
            cross_out.at[k, h], cross_in.at[k, h], cross_send.at[k, h], cross_recv.at[k, h], 0, cross
        )

    def near_sum(d, h):
        return remote(
            result.at[2 * d + 1, h], plane_in.at[d, h], near_send.at[d, h], near_recv.at[d, h], 1, tp
        )

    def plane_sum(d, h):
        return remote(
            sum_out.at[d - 1, h], sum_in.at[d - 1, h], sum_send.at[d, h], sum_recv.at[d, h], 2 * d, tp
        )

    weights = [
        pltpu.make_async_copy(src, dst, w_sem.at[i])
        for i, (src, dst) in enumerate(((gate_hbm, gate_w), (up_hbm, up_w), (down_hbm, down_w)))
    ]
    barrier = pltpu.get_barrier_semaphore()
    peers = [(partner(2 * d), tp) for d in range(1, PLANES)]
    peers += [(partner(1), tp), (me, cross), (me, core)]
    for peer in peers:
        pl.semaphore_signal(barrier, inc=1, device_id=peer, device_id_type=MESH)

    fetch.wait()
    for copy in weights:
        copy.start()
    values = token_in[...].astype(f32)
    scale = lax.rsqrt(jnp.mean(values * values, axis=-1, keepdims=True) + NORM_EPS)
    for j in range(4):
        for h in range(PARTS):
            span = slice(j * quarter + h * width, j * quarter + (h + 1) * width)
            normed[j, h] = (token_in[:, span].astype(f32) * scale * gain[:, span]).astype(bf16)
    meta[0, 0:2] = ids[...].astype(f32)
    meta[0, 2:4] = route[...]
    pl.semaphore_wait(barrier, len(peers))
    for d in range(1, PLANES):
        describe(d).start()

    def L(d, h):
        for q in shares(d, h):
            spread(d, q, h).start()

    def M(d):
        if d:
            describe(d).wait_recv()
        else:
            earlier = lax.broadcasted_iota(jnp.int32, (tok_count, tok_count), 0)
            later = lax.broadcasted_iota(jnp.int32, (tok_count, tok_count), 1)
            before[...] = jnp.where(earlier < later, 1.0, 0.0).astype(bf16)
        for side in range(2):
            hits = meta[d, 0:2] == partner(side).astype(f32)
            named = jnp.sum(jnp.where(hits, 1.0, 0.0), axis=0, keepdims=True)
            weight = jnp.sum(jnp.where(hits, meta[d, 2:4], 0.0), axis=0, keepdims=True)
            count = jnp.dot(
                jnp.broadcast_to(named, (8, tok_count)).astype(bf16),
                before[...],
                preferred_element_type=f32,
            )[0:1]
            slot = jnp.where(named > 0.0, count.astype(jnp.int32), -1)
            place = lax.broadcasted_iota(jnp.int32, (slots, tok_count), 0)
            chosen = place == slot
            mix = jnp.where(chosen, weight, 0.0)
            mix_high = mix.astype(bf16)
            high[d, side] = mix_high
            low[d, side] = (mix - mix_high.astype(f32)).astype(bf16)
            picker[d, side] = jnp.where(chosen, 1.0, 0.0).astype(bf16)

    def block(d, q, h):
        return dense[d - 1, q, h] if d else normed[quarters[q], h]

    def pick(d, side, source):
        return jnp.dot(picker[d, side], source, preferred_element_type=f32).astype(bf16)

    arrived = set()

    def arrive(d, h):
        if d and (d, h) not in arrived:
            arrived.add((d, h))
            for q in shares(d, h):
                spread(d, q, h).wait_recv()

    def A(d, h):
        if d == 0:
            for j in range(4):
                for n in range(PARTS):
                    rows[0, j, n] = pick(0, 0, normed[j, n])
            return
        arrive(d, h)
        for q in shares(d, h):
            rows[2 * d, quarters[q], h] = pick(d, 0, block(d, q, h))
            to_core(2 * d, q, h).start()
        if len(shares(d, h)) == 1:
            to_cross(2 * d, h).start()

    def Y(d, h):
        arrive(d, h)
        for n in range(PARTS) if d == 0 else (h,):
            for q in shares(d, n):
                picked[d, q, n] = pick(d, 1, block(d, q, n))
                neighbour(d, q, n).start()

    def B(d, h):
        k = 2 * d + 1
        for q in shares(d, h):
            neighbour(d, q, h).wait_recv()
            to_core(k, q, h).start()
        if len(shares(d, h)) == 1:
            to_cross(k, h).start()

    def X(d, side, h):
        k = 2 * d + side
        to_cross(k, h).wait_recv()
        to_core(k, 1, h).start()

    def F(d, side):
        k = 2 * d + side
        if (d, side) == FIRST:
            for copy in weights:
                copy.wait()
        if k:
            for q in range(2):
                for h in range(PARTS):
                    to_core(k, q, h).wait_recv()
        whole = jnp.concatenate([rows[k, j, h] for j in range(4) for h in range(PARTS)], axis=1)
        gate_sum = jnp.dot(whole, gate_w[...], preferred_element_type=f32)
        up_sum = jnp.dot(whole, up_w[...], preferred_element_type=f32)
        activated = activate(gate_sum, up_sum)
        for j in range(4):
            piece = jnp.dot(
                activated, down_w[:, j * quarter : (j + 1) * quarter], preferred_element_type=f32
            ).astype(bf16)
            for h in range(PARTS):
                part[k, j % 2, h, j // 2] = piece[:, h * width : (h + 1) * width]
        for h in range(PARTS):
            pair(k, h).start()

    def G(d, side, h):
        k = 2 * d + side
        pair(k, h).wait_recv()
        both = part[k, b, h, 1 - a].astype(f32) + pair_in[k, h, 1 - a].astype(f32)
        cross_out[k, h] = both.astype(bf16)
        cross_sum(k, h).start()

    def H(d, side, h):
        k = 2 * d + side
        cross_sum(k, h).wait_recv()
        both = part[k, b, h, a].astype(f32) + pair_in[k, h, a].astype(f32)
        result[k, h] = (both + cross_in[k, h].astype(f32)).astype(bf16)
        if side:
            near_sum(d, h).start()

    def S(d, h):
        near_sum(d, h).wait_recv()
        mixed = 0.0
        for side, value in ((0, result[2 * d, h]), (1, plane_in[d, h])):
            for share in (high, low):
                mixed += lax.dot_general(
                    share[d, side], value, (((0,), (0,)), ((), ())), preferred_element_type=f32
                )
        if d:
            sum_out[d - 1, h] = mixed.astype(bf16)
            plane_sum(d, h).start()
        else:
            total[h] = mixed

    def J(d, h):
        plane_sum(d, h).wait_recv()

    stages = dict(L=L, M=M, A=A, Y=Y, B=B, X=X, F=F, G=G, H=H, S=S, J=J)
    for step in STEPS:
        stages[step[0]](*(int(n) for n in step[1:]))

    def store(h):
        span = pl.ds(h * width, width)
        return pltpu.make_async_copy(out_part.at[h], out.at[:, span], io_sem.at[h])

    for h in range(PARTS):
        mixed = total[h]
        for d in range(1, PLANES):
            mixed += sum_in[d - 1, h].astype(f32)
        out_part[h] = mixed.astype(bf16)
        store(h).start()

    for d in range(PLANES):
        if d:
            describe(d).wait_send()
        for h in range(PARTS):
            for q in shares(d, h):
                neighbour(d, q, h).wait_send()
                if d:
                    spread(d, q, h).wait_send()
            near_sum(d, h).wait_send()
            if d:
                plane_sum(d, h).wait_send()
    for h in range(PARTS):
        store(h).wait()
    for k in range(groups):
        for h in range(PARTS):
            pair(k, h).wait_send()
            cross_sum(k, h).wait_send()
            if k:
                for q in range(2):
                    to_core(k, q, h).wait_send()
            if len(shares(k // 2, h)) == 1:
                to_cross(k, h).wait_send()


FIRST = next((int(step[1]), int(step[2])) for step in STEPS if step[0] == "F")


def plane_call(groups, capacity, operands):
    tokens, weights = operands[0], operands[4:]
    tok_count, model_width = tokens.shape
    quarter = model_width // 4
    width = quarter // PARTS
    bf16, f32 = jnp.bfloat16, jnp.float32
    compact = (PARTS, capacity, width)
    full = (PARTS, tok_count, width)
    dma = pltpu.SemaphoreType.DMA
    return pl.pallas_call(
        functools.partial(plane_kernel, groups),
        out_shape=jax.ShapeDtypeStruct((tok_count, quarter), bf16),
        in_specs=[pl.BlockSpec(memory_space=pl.ANY)]
        + [pl.BlockSpec(memory_space=pltpu.VMEM)] * 3
        + [pl.BlockSpec(memory_space=pl.ANY)] * 3,
        out_specs=pl.BlockSpec(memory_space=pl.ANY),
        scratch_shapes=[
            *[pltpu.VMEM(weight.shape, bf16) for weight in weights],
            pltpu.VMEM(tokens.shape, bf16),
            pltpu.VMEM(full, bf16),
            pltpu.VMEM((tok_count, tok_count), bf16),
            pltpu.VMEM((PLANES, 8, tok_count), f32),
            pltpu.VMEM((4, *full), bf16),
            pltpu.VMEM((PLANES - 1, 2, *full), bf16),
            *[pltpu.VMEM((PLANES, 2, capacity, tok_count), bf16)] * 3,
            pltpu.VMEM((groups, 4, *compact), bf16),
            pltpu.VMEM((PLANES, 2, *compact), bf16),
            pltpu.VMEM((groups, 2, PARTS, 2, capacity, width), bf16),
            pltpu.VMEM((groups, PARTS, 2, capacity, width), bf16),
            *[pltpu.VMEM((groups, *compact), bf16)] * 3,
            pltpu.VMEM((PLANES, *compact), bf16),
            pltpu.VMEM(full, f32),
            *[pltpu.VMEM((PLANES - 1, *full), bf16)] * 2,
            dma((3,)),
            dma((PARTS + 1,)),
            *[dma((PLANES,))] * 2,
            *[dma((PLANES, 2, PARTS))] * 4,
            *[dma((groups, 2, PARTS))] * 2,
            *[dma((groups, PARTS))] * 6,
            *[dma((PLANES, PARTS))] * 4,
        ],
        compiler_params=pltpu.CompilerParams(
            collective_id=0, has_side_effects=True, vmem_limit_bytes=60 * 1024 * 1024
        ),
    )(*operands)


def expert_kernel(
    groups,
    tokens,
    ids,
    route,
    gain,
    gate_hbm,
    up_hbm,
    down_hbm,
    out,
    gate_w,
    up_w,
    down_w,
    normed_own,
    normed_cross,
    before,
    send,
    send_cross,
    back,
    high,
    low,
    total_out,
    rows,
    part,
    pair_in,
    cross_out,
    cross_in,
    result,
    w_sem,
    disp_send,
    disp_recv,
    cross_send,
    cross_recv,
    core_send,
    core_recv,
    fwd_send,
    fwd_recv,
    pair_send,
    pair_recv,
    sum_send,
    sum_recv,
    ret_send,
    ret_recv,
):
    me = lax.axis_index("ep")
    tp = lax.axis_index("tp")
    a, b = tp // 2, lax.rem(tp, 2)
    cross = 2 * (1 - a) + b
    core = 2 * a + 1 - b
    capacity, quarter = send.shape[1:]
    tok_count = tokens.shape[0]
    half = groups // 2

    weights = [
        pltpu.make_async_copy(src, dst, w_sem.at[i])
        for i, (src, dst) in enumerate(((gate_hbm, gate_w), (up_hbm, up_w), (down_hbm, down_w)))
    ]

    def remote(src, dst, send_sem, recv_sem, ep_index, tp_index):
        return pltpu.make_async_remote_copy(
            src_ref=src,
            dst_ref=dst,
            send_sem=send_sem,
            recv_sem=recv_sem,
            device_id=(ep_index, tp_index),
            device_id_type=MESH,
        )

    def partner(k):
        total, bit = 0, 1
        while bit < groups:
            total += bit * lax.rem(me // bit + k // bit, 2)
            bit *= 2
        return total

    def order(i):
        i = i + (i // (groups - 2)) * (1 - 2 * lax.rem(i, 2))
        return i // 2 + half * lax.rem(i, 2)

    def dispatch(k):
        dst = partner(k)
        return remote(send.at[k], rows.at[k, tp], disp_send.at[k], disp_recv.at[k], dst, tp)

    def dispatch_cross(k):
        dst = partner(k)
        return remote(
            send_cross.at[k],
            rows.at[k, cross],
            cross_send.at[k],
            cross_recv.at[k],
            dst,
            tp,
        )

    def to_cross(k):
        return remote(rows.at[k, tp], rows.at[k, tp], cross_send.at[k], cross_recv.at[k], me, cross)

    def to_core(k):
        return remote(rows.at[k, tp], rows.at[k, tp], core_send.at[k], core_recv.at[k], me, core)

    def forward(k):
        return remote(rows.at[k, cross], rows.at[k, cross], fwd_send.at[k], fwd_recv.at[k], me, core)

    def pair(k):
        return remote(part.at[k, 1 - b], pair_in.at[k], pair_send.at[k], pair_recv.at[k], me, core)

    def cross_sum(k):
        return remote(cross_out.at[k], cross_in.at[k], sum_send.at[k], sum_recv.at[k], me, cross)

    def give_back(k):
        return remote(result.at[k], back.at[k], ret_send.at[k], ret_recv.at[k], partner(k), tp)

    for copy in weights:
        copy.start()

    barrier = pltpu.get_barrier_semaphore()

    def greet(k, carry):
        pl.semaphore_signal(
            barrier, inc=1, device_id=(lax.rem(me + k, groups), tp), device_id_type=MESH
        )
        return carry

    lax.fori_loop(1, groups, greet, 0)
    pl.semaphore_signal(barrier, inc=1, device_id=(me, cross), device_id_type=MESH)
    pl.semaphore_signal(barrier, inc=1, device_id=(me, core), device_id_type=MESH)

    values = tokens[...].astype(jnp.float32)
    scale = lax.rsqrt(jnp.mean(values * values, axis=-1, keepdims=True) + NORM_EPS)

    def normed(index):
        span = pl.ds(pl.multiple_of(index * quarter, quarter), quarter)
        return (tokens[:, span].astype(jnp.float32) * scale * gain[:, span]).astype(jnp.bfloat16)

    normed_own[...] = normed(tp)
    normed_cross[...] = normed(cross)
    earlier = lax.broadcasted_iota(jnp.int32, (tok_count, tok_count), 0)
    later = lax.broadcasted_iota(jnp.int32, (tok_count, tok_count), 1)
    before[...] = jnp.where(earlier < later, 1.0, 0.0).astype(jnp.bfloat16)

    def select(k):
        expert = partner(k)
        hits = ids[...] == expert
        named = jnp.sum(jnp.where(hits, 1.0, 0.0), axis=0, keepdims=True)
        weight = jnp.sum(jnp.where(hits, route[...], 0.0), axis=0, keepdims=True)
        count = jnp.dot(
            jnp.broadcast_to(named, (8, tok_count)).astype(jnp.bfloat16),
            before[...],
            preferred_element_type=jnp.float32,
        )[0:1]
        slot = jnp.where(named > 0.0, count.astype(jnp.int32), -1)
        place = lax.broadcasted_iota(jnp.int32, (capacity, tok_count), 0)
        chosen = place == slot
        mix = jnp.where(chosen, weight, 0.0)
        mix_high = mix.astype(jnp.bfloat16)
        high[k] = mix_high
        low[k] = (mix - mix_high.astype(jnp.float32)).astype(jnp.bfloat16)
        return jnp.where(chosen, 1.0, 0.0).astype(jnp.bfloat16)

    def pick(chosen, source):
        return jnp.dot(chosen, source[...], preferred_element_type=jnp.float32).astype(jnp.bfloat16)

    chosen = select(0)
    rows[0, tp] = pick(chosen, normed_own)
    rows[0, cross] = pick(chosen, normed_cross)
    pl.semaphore_wait(barrier, groups + 1)

    def launch(i, carry):
        k = order(i)
        chosen = select(k)
        send[k] = pick(chosen, normed_own)
        dispatch(k).start()

        @pl.when(k < half)
        def _():
            send_cross[k] = pick(chosen, normed_cross)
            dispatch_cross(k).start()

        return carry

    lax.fori_loop(1, groups, launch, 0)
    for copy in weights:
        copy.wait()

    def step(i, carry):
        @pl.when(i >= 4)
        def _():
            k = order(i - 4)
            cross_sum(k).wait_recv()
            total = part[k, b, a].astype(jnp.float32) + pair_in[k, a].astype(jnp.float32)
            total = (total + cross_in[k].astype(jnp.float32)).astype(jnp.bfloat16)

            @pl.when(k == 0)
            def _():
                back[0] = total

            @pl.when(k > 0)
            def _():
                result[k] = total
                give_back(k).start()

        @pl.when((i >= 3) & (i < groups + 3))
        def _():
            k = order(i - 3)
            pair(k).wait_recv()
            total = part[k, b, 1 - a].astype(jnp.float32) + pair_in[k, 1 - a].astype(jnp.float32)
            cross_out[k] = total.astype(jnp.bfloat16)
            cross_sum(k).start()

        @pl.when((i >= 2) & (i < groups + 2))
        def _():
            k = order(i - 2)
            to_core(k).wait_recv()
            forward(k).wait_recv()
            block = jnp.concatenate([rows[k, j] for j in range(4)], axis=1)
            gate_sum = jnp.dot(block, gate_w[...], preferred_element_type=jnp.float32)
            up_sum = jnp.dot(block, up_w[...], preferred_element_type=jnp.float32)
            activated = activate(gate_sum, up_sum)
            for j in range(4):
                part[k, j % 2, j // 2] = jnp.dot(
                    activated,
                    down_w[:, j * quarter : (j + 1) * quarter],
                    preferred_element_type=jnp.float32,
                ).astype(jnp.bfloat16)
            pair(k).start()

        @pl.when((i >= 1) & (i < groups + 1))
        def _():
            k = order(i - 1)

            @pl.when(k > 0)
            def _():
                to_cross(k).wait_recv()

            forward(k).start()

        @pl.when(i < groups)
        def _():
            k = order(i)

            @pl.when(k > 0)
            def _():
                dispatch(k).wait_recv()

            @pl.when(k >= half)
            def _():
                to_cross(k).start()

            to_core(k).start()

        return carry

    lax.fori_loop(0, groups + 4, step, 0)

    total_out[...] = jnp.zeros_like(total_out)

    def finish(i, carry):
        k = order(i)

        @pl.when(k > 0)
        def _():
            give_back(k).wait_recv()

        for share in (high, low):
            total_out[...] += lax.dot_general(
                share[k], back[k], (((0,), (0,)), ((), ())), preferred_element_type=jnp.float32
            )
        return carry

    lax.fori_loop(0, groups, finish, 0)
    out[...] = total_out[...].astype(jnp.bfloat16)

    def drain(k, carry):
        to_core(k).wait_send()
        forward(k).wait_send()
        pair(k).wait_send()
        cross_sum(k).wait_send()

        @pl.when(k > 0)
        def _():
            to_cross(k).wait_send()
            dispatch(k).wait_send()
            give_back(k).wait_send()

        return carry

    lax.fori_loop(0, groups, drain, 0)


def shards(tokens, expert_ids, route_weight, norm_gain, expert_gate, expert_up, expert_down):
    groups = lax.axis_size("ep")
    tp_count = lax.axis_size("tp")
    experts = groups * expert_gate.shape[0]
    tok_count, model_width = tokens.shape
    top_count = expert_ids.shape[1]
    capacity = min(tok_count, 3 * tok_count * top_count // experts)
    quarter = model_width // tp_count
    bf16 = jnp.bfloat16
    slots = (groups, capacity, quarter)
    weights = (expert_gate[0], expert_up[0], expert_down[0])
    operands = (tokens, expert_ids.T, route_weight.T, norm_gain[None, :], *weights)
    if groups == 2 * PLANES and 2 * capacity > tok_count:
        return plane_call(groups, capacity, operands)
    return pl.pallas_call(
        functools.partial(expert_kernel, groups),
        out_shape=jax.ShapeDtypeStruct((tok_count, quarter), bf16),
        in_specs=[pl.BlockSpec(memory_space=pltpu.VMEM)] * 4
        + [pl.BlockSpec(memory_space=pl.ANY)] * 3,
        out_specs=pl.BlockSpec(memory_space=pltpu.VMEM),
        scratch_shapes=[
            *[pltpu.VMEM(weight.shape, bf16) for weight in weights],
            pltpu.VMEM((tok_count, quarter), bf16),
            pltpu.VMEM((tok_count, quarter), bf16),
            pltpu.VMEM((tok_count, tok_count), bf16),
            pltpu.VMEM(slots, bf16),
            pltpu.VMEM((groups // 2, capacity, quarter), bf16),
            pltpu.VMEM(slots, bf16),
            pltpu.VMEM((groups, capacity, tok_count), bf16),
            pltpu.VMEM((groups, capacity, tok_count), bf16),
            pltpu.VMEM((tok_count, quarter), jnp.float32),
            pltpu.VMEM((groups, 4, capacity, quarter), bf16),
            pltpu.VMEM((groups, 2, 2, capacity, quarter), bf16),
            pltpu.VMEM((groups, 2, capacity, quarter), bf16),
            pltpu.VMEM(slots, bf16),
            pltpu.VMEM(slots, bf16),
            pltpu.VMEM(slots, bf16),
            pltpu.SemaphoreType.DMA((3,)),
            *[pltpu.SemaphoreType.DMA((groups,)) for _ in range(14)],
        ],
        compiler_params=pltpu.CompilerParams(
            collective_id=0, has_side_effects=True, vmem_limit_bytes=60 * 1024 * 1024
        ),
    )(*operands)


def solution(mesh):
    return jax.shard_map(
        shards,
        mesh=mesh,
        in_specs=(
            P("ep", None),
            P("ep", None),
            P("ep", None),
            P(),
            P("ep", None, "tp"),
            P("ep", None, "tp"),
            P("ep", "tp", None),
        ),
        out_specs=P("ep", "tp"),
        check_vma=False,
    )
```

```python
import functools

import jax
import jax.numpy as jnp
from jax import lax
from jax.experimental import pallas as pl
from jax.experimental.pallas import tpu as pltpu
from jax.sharding import PartitionSpec as P

NORM_EPS = 1e-06
CLAMP_LIMIT = 7.0
SWISH_SCALE = 1.702
MESH = pl.DeviceIdType.MESH
STEPS = (
    "L31", "L30", "L10", "M0", "Y00", "L21", "M3", "Y31", "B01", "B00",
    "L11", "A31", "B31", "A30", "Y30", "F01", "M1", "Y10", "L20", "G010",
    "B30", "X301", "M2", "Y21", "X311", "A21", "X300", "F30", "Y11", "G300",
    "X310", "B10", "A11", "B21", "F31", "G311", "A10", "Y20", "H300", "G310",
    "B11", "G301", "F10", "F11", "A20", "H311", "G100", "G110", "X211", "X201",
    "G111", "H310", "B20", "F21", "H301", "S31", "G210", "H110", "G211", "S30",
    "H010", "F20", "G200", "G101", "G201", "H210", "H100", "S10", "A00", "F00",
    "H111", "H200", "S20", "J31", "G011", "H211", "G000", "J30", "H101", "S11",
    "H201", "S21", "J10", "H011", "G001", "H001", "J20", "S01", "J11", "H000",
    "S00", "J21",
)
CARRIED = ((2, 2), (2, 2), (2, 1), (1, 1))
PLANES, PARTS = len(CARRIED), len(CARRIED[0])


def activate(gate_sum, up_sum):
    gate_cut = jnp.minimum(gate_sum, CLAMP_LIMIT)
    up_cut = jnp.clip(up_sum, -CLAMP_LIMIT, CLAMP_LIMIT)
    return ((up_cut + 1.0) * gate_cut * jax.nn.sigmoid(SWISH_SCALE * gate_cut)).astype(jnp.bfloat16)


def plane_kernel(
    groups,
    tokens,
    ids,
    route,
    gain,
    gate_hbm,
    up_hbm,
    down_hbm,
    out,
    gate_w,
    up_w,
    down_w,
    token_in,
    before,
    meta,
    normed,
    dense,
    picker,
    high,
    low,
    rows,
    picked,
    part,
    pair_in,
    cross_out,
    cross_in,
    result,
    plane_in,
    total,
    sum_out,
    sum_in,
    w_sem,
    io_sem,
    meta_send,
    meta_recv,
    dense_send,
    dense_recv,
    pick_send,
    pick_recv,
    core_send,
    core_recv,
    fwd_send,
    fwd_recv,
    pair_send,
    pair_recv,
    cross_send,
    cross_recv,
    near_send,
    near_recv,
    sum_send,
    sum_recv,
):
    me = lax.axis_index("ep")
    tp = lax.axis_index("tp")
    a, b = tp // 2, lax.rem(tp, 2)
    cross = 2 * (1 - a) + b
    core = 2 * a + 1 - b
    quarters = (tp, cross)
    slots, width = rows.shape[3:]
    quarter = PARTS * width
    tok_count = tokens.shape[0]
    f32, bf16 = jnp.float32, jnp.bfloat16
    fetch = pltpu.make_async_copy(tokens, token_in, io_sem)
    fetch.start()

    def partner(k):
        total, bit = 0, 1
        while bit < groups:
            total += bit * lax.rem(me // bit + k // bit, 2)
            bit *= 2
        return total

    def remote(src, dst, send_sem, recv_sem, k, tp_index):
        return pltpu.make_async_remote_copy(
            src_ref=src,
            dst_ref=dst,
            send_sem=send_sem,
            recv_sem=recv_sem,
            device_id=(partner(k), tp_index),
            device_id_type=MESH,
        )

    def shares(d, h):
        return range(CARRIED[d][h])

    def settle(ref, sem):
        pltpu.make_async_copy(ref, ref, sem).wait()

    def describe(d):
        return remote(meta.at[0], meta.at[d], meta_send, meta_recv.at[d], 2 * d, tp)

    def spread(d, q, h):
        return remote(
            normed.at[quarters[q], h],
            dense.at[d - 1, q, h],
            dense_send.at[d, h],
            dense_recv.at[d, h],
            2 * d,
            tp,
        )

    def neighbour(d, q, h):
        return remote(
            picked.at[d, q, h],
            rows.at[2 * d + 1, quarters[q], h],
            pick_send.at[d, h],
            pick_recv.at[d, h],
            1,
            tp,
        )

    def to_core(k, q, h):
        ref = rows.at[k, quarters[q], h]
        return remote(ref, ref, core_send, core_recv.at[k], 0, core)

    def to_cross(k, h):
        ref = rows.at[k, tp, h]
        return remote(ref, ref, fwd_send, fwd_recv.at[k - PLANES, h], 0, cross)

    def pair(k, h):
        return remote(
            part.at[k, 1 - b, h], pair_in.at[k, h], pair_send, pair_recv.at[k, h], 0, core
        )

    def cross_sum(k, h):
        return remote(
            cross_out.at[k, h], cross_in.at[k, h], cross_send, cross_recv.at[k, h], 0, cross
        )

    def near_sum(d, h):
        return remote(
            result.at[2 * d + 1, h], plane_in.at[d, h], near_send, near_recv.at[d, h], 1, tp
        )

    def plane_sum(d, h):
        return remote(
            sum_out.at[d - 1, h], sum_in.at[d - 1, h], sum_send, sum_recv.at[d, h], 2 * d, tp
        )

    weights = [
        pltpu.make_async_copy(src, dst, w_sem.at[i])
        for i, (src, dst) in enumerate(((gate_hbm, gate_w), (up_hbm, up_w), (down_hbm, down_w)))
    ]
    barrier = pltpu.get_barrier_semaphore()
    peers = [(partner(2 * d), tp) for d in range(1, PLANES)]
    peers += [(partner(1), tp), (me, cross), (me, core)]
    for peer in peers:
        pl.semaphore_signal(barrier, inc=1, device_id=peer, device_id_type=MESH)

    fetch.wait()
    for copy in weights:
        copy.start()
    values = token_in[...].astype(f32)
    scale = lax.rsqrt(jnp.mean(values * values, axis=-1, keepdims=True) + NORM_EPS)
    for j in range(4):
        for h in range(PARTS):
            span = slice(j * quarter + h * width, j * quarter + (h + 1) * width)
            normed[j, h] = (token_in[:, span].astype(f32) * scale * gain[:, span]).astype(bf16)
    meta[0, 0:2] = ids[...].astype(f32)
    meta[0, 2:4] = route[...]
    pl.semaphore_wait(barrier, len(peers))
    for d in range(1, PLANES):
        describe(d).start()

    def L(d, h):
        for q in shares(d, h):
            spread(d, q, h).start()

    def M(d):
        if d:
            describe(d).wait_recv()
        else:
            earlier = lax.broadcasted_iota(jnp.int32, (tok_count, tok_count), 0)
            later = lax.broadcasted_iota(jnp.int32, (tok_count, tok_count), 1)
            before[...] = jnp.where(earlier < later, 1.0, 0.0).astype(bf16)
        for side in range(2):
            hits = meta[d, 0:2] == partner(side).astype(f32)
            named = jnp.sum(jnp.where(hits, 1.0, 0.0), axis=0, keepdims=True)
            weight = jnp.sum(jnp.where(hits, meta[d, 2:4], 0.0), axis=0, keepdims=True)
            count = jnp.dot(
                jnp.broadcast_to(named, (8, tok_count)).astype(bf16),
                before[...],
                preferred_element_type=f32,
            )[0:1]
            slot = jnp.where(named > 0.0, count.astype(jnp.int32), -1)
            place = lax.broadcasted_iota(jnp.int32, (slots, tok_count), 0)
            chosen = place == slot
            mix = jnp.where(chosen, weight, 0.0)
            mix_high = mix.astype(bf16)
            high[d, side] = mix_high
            low[d, side] = (mix - mix_high.astype(f32)).astype(bf16)
            picker[d, side] = jnp.where(chosen, 1.0, 0.0).astype(bf16)

    def block(d, q, h):
        return dense[d - 1, q, h] if d else normed[quarters[q], h]

    def pick(d, side, source):
        return jnp.dot(picker[d, side], source, preferred_element_type=f32).astype(bf16)

    arrived = set()

    def arrive(d, h):
        if d and (d, h) not in arrived:
            arrived.add((d, h))
            settle(dense.at[d - 1, 0 : CARRIED[d][h], h], dense_recv.at[d, h])

    def A(d, h):
        if d == 0:
            for j in range(4):
                for n in range(PARTS):
                    rows[0, j, n] = pick(0, 0, normed[j, n])
            return
        arrive(d, h)
        for q in shares(d, h):
            rows[2 * d, quarters[q], h] = pick(d, 0, block(d, q, h))
            to_core(2 * d, q, h).start()
        if len(shares(d, h)) == 1:
            to_cross(2 * d, h).start()

    def Y(d, h):
        arrive(d, h)
        for n in range(PARTS) if d == 0 else (h,):
            for q in shares(d, n):
                picked[d, q, n] = pick(d, 1, block(d, q, n))
                neighbour(d, q, n).start()

    def B(d, h):
        k = 2 * d + 1
        settle(picked.at[d, 0 : CARRIED[d][h], h], pick_recv.at[d, h])
        for q in shares(d, h):
            to_core(k, q, h).start()
        if len(shares(d, h)) == 1:
            to_cross(k, h).start()

    def X(d, side, h):
        k = 2 * d + side
        to_cross(k, h).wait_recv()
        to_core(k, 1, h).start()

    def F(d, side):
        k = 2 * d + side
        if (d, side) == FIRST:
            for copy in weights:
                copy.wait()
        if k:
            settle(rows.at[k, 0:2], core_recv.at[k])
        whole = jnp.concatenate([rows[k, j, h] for j in range(4) for h in range(PARTS)], axis=1)
        gate_sum = jnp.dot(whole, gate_w[...], preferred_element_type=f32)
        up_sum = jnp.dot(whole, up_w[...], preferred_element_type=f32)
        activated = activate(gate_sum, up_sum)
        for j in range(4):
            piece = jnp.dot(
                activated, down_w[:, j * quarter : (j + 1) * quarter], preferred_element_type=f32
            ).astype(bf16)
            for h in range(PARTS):
                part[k, j % 2, h, j // 2] = piece[:, h * width : (h + 1) * width]
        for h in range(PARTS):
            pair(k, h).start()

    def G(d, side, h):
        k = 2 * d + side
        pair(k, h).wait_recv()
        both = part[k, b, h, 1 - a].astype(f32) + pair_in[k, h, 1 - a].astype(f32)
        cross_out[k, h] = both.astype(bf16)
        cross_sum(k, h).start()

    def H(d, side, h):
        k = 2 * d + side
        cross_sum(k, h).wait_recv()
        both = part[k, b, h, a].astype(f32) + pair_in[k, h, a].astype(f32)
        result[k, h] = (both + cross_in[k, h].astype(f32)).astype(bf16)
        if side:
            near_sum(d, h).start()

    def S(d, h):
        near_sum(d, h).wait_recv()
        mixed = 0.0
        for side, value in ((0, result[2 * d, h]), (1, plane_in[d, h])):
            for share in (high, low):
                mixed += lax.dot_general(
                    share[d, side], value, (((0,), (0,)), ((), ())), preferred_element_type=f32
                )
        if d:
            sum_out[d - 1, h] = mixed.astype(bf16)
            plane_sum(d, h).start()
        else:
            total[h] = mixed

    def J(d, h):
        plane_sum(d, h).wait_recv()

    stages = dict(L=L, M=M, A=A, Y=Y, B=B, X=X, F=F, G=G, H=H, S=S, J=J)
    for step in STEPS:
        stages[step[0]](*(int(n) for n in step[1:]))

    for h in range(PARTS):
        mixed = total[h]
        for d in range(1, PLANES):
            mixed += sum_in[d - 1, h].astype(f32)
        out[:, h * width : (h + 1) * width] = mixed.astype(bf16)

    settle(meta.at[1:PLANES], meta_send)
    for d in range(PLANES):
        for h in range(PARTS):
            settle(picked.at[d, 0 : CARRIED[d][h], h], pick_send.at[d, h])
            if d:
                settle(dense.at[d - 1, 0 : CARRIED[d][h], h], dense_send.at[d, h])
    settle(rows.at[1:groups, 0:2], core_send)
    settle(rows.at[0 : sum(carry.count(1) for carry in CARRIED) * 2 // PARTS, 0], fwd_send)
    settle(part.at[:, 0], pair_send)
    settle(cross_out, cross_send)
    settle(plane_in, near_send)
    settle(sum_out, sum_send)


FIRST = next((int(step[1]), int(step[2])) for step in STEPS if step[0] == "F")


def plane_call(groups, capacity, operands):
    tokens, weights = operands[0], operands[4:]
    tok_count, model_width = tokens.shape
    quarter = model_width // 4
    width = quarter // PARTS
    bf16, f32 = jnp.bfloat16, jnp.float32
    compact = (PARTS, capacity, width)
    full = (PARTS, tok_count, width)
    dma = pltpu.SemaphoreType.DMA
    return pl.pallas_call(
        functools.partial(plane_kernel, groups),
        out_shape=pltpu.VMEM((tok_count, quarter), bf16),
        in_specs=[pl.BlockSpec(memory_space=pl.ANY)]
        + [pl.BlockSpec(memory_space=pltpu.VMEM)] * 3
        + [pl.BlockSpec(memory_space=pl.ANY)] * 3,
        out_specs=pl.BlockSpec(memory_space=pltpu.VMEM),
        scratch_shapes=[
            *[pltpu.VMEM(weight.shape, bf16) for weight in weights],
            pltpu.VMEM(tokens.shape, bf16),
            pltpu.VMEM((tok_count, tok_count), bf16),
            pltpu.VMEM((PLANES, 8, tok_count), f32),
            pltpu.VMEM((4, *full), bf16),
            pltpu.VMEM((PLANES - 1, 2, *full), bf16),
            *[pltpu.VMEM((PLANES, 2, capacity, tok_count), bf16)] * 3,
            pltpu.VMEM((groups, 4, *compact), bf16),
            pltpu.VMEM((PLANES, 2, *compact), bf16),
            pltpu.VMEM((groups, 2, PARTS, 2, capacity, width), bf16),
            pltpu.VMEM((groups, PARTS, 2, capacity, width), bf16),
            *[pltpu.VMEM((groups, *compact), bf16)] * 3,
            pltpu.VMEM((PLANES, *compact), bf16),
            pltpu.VMEM(full, f32),
            *[pltpu.VMEM((PLANES - 1, *full), bf16)] * 2,
            dma((3,)),
            dma,
            dma,
            dma((PLANES,)),
            *[dma((PLANES, PARTS))] * 4,
            dma,
            dma((groups,)),
            dma,
            dma((groups - PLANES, PARTS)),
            dma,
            dma((groups, PARTS)),
            dma,
            dma((groups, PARTS)),
            dma,
            dma((PLANES, PARTS)),
            dma,
            dma((PLANES, PARTS)),
        ],
        compiler_params=pltpu.CompilerParams(
            collective_id=0, has_side_effects=True, vmem_limit_bytes=60 * 1024 * 1024
        ),
    )(*operands)


def expert_kernel(
    groups,
    tokens,
    ids,
    route,
    gain,
    gate_hbm,
    up_hbm,
    down_hbm,
    out,
    gate_w,
    up_w,
    down_w,
    normed_own,
    normed_cross,
    before,
    send,
    send_cross,
    back,
    high,
    low,
    total_out,
    rows,
    part,
    pair_in,
    cross_out,
    cross_in,
    result,
    w_sem,
    disp_send,
    disp_recv,
    cross_send,
    cross_recv,
    core_send,
    core_recv,
    fwd_send,
    fwd_recv,
    pair_send,
    pair_recv,
    sum_send,
    sum_recv,
    ret_send,
    ret_recv,
):
    me = lax.axis_index("ep")
    tp = lax.axis_index("tp")
    a, b = tp // 2, lax.rem(tp, 2)
    cross = 2 * (1 - a) + b
    core = 2 * a + 1 - b
    capacity, quarter = send.shape[1:]
    tok_count = tokens.shape[0]
    half = groups // 2

    weights = [
        pltpu.make_async_copy(src, dst, w_sem.at[i])
        for i, (src, dst) in enumerate(((gate_hbm, gate_w), (up_hbm, up_w), (down_hbm, down_w)))
    ]

    def remote(src, dst, send_sem, recv_sem, ep_index, tp_index):
        return pltpu.make_async_remote_copy(
            src_ref=src,
            dst_ref=dst,
            send_sem=send_sem,
            recv_sem=recv_sem,
            device_id=(ep_index, tp_index),
            device_id_type=MESH,
        )

    def partner(k):
        total, bit = 0, 1
        while bit < groups:
            total += bit * lax.rem(me // bit + k // bit, 2)
            bit *= 2
        return total

    def order(i):
        i = i + (i // (groups - 2)) * (1 - 2 * lax.rem(i, 2))
        return i // 2 + half * lax.rem(i, 2)

    def dispatch(k):
        dst = partner(k)
        return remote(send.at[k], rows.at[k, tp], disp_send.at[k], disp_recv.at[k], dst, tp)

    def dispatch_cross(k):
        dst = partner(k)
        return remote(
            send_cross.at[k],
            rows.at[k, cross],
            cross_send.at[k],
            cross_recv.at[k],
            dst,
            tp,
        )

    def to_cross(k):
        return remote(rows.at[k, tp], rows.at[k, tp], cross_send.at[k], cross_recv.at[k], me, cross)

    def to_core(k):
        return remote(rows.at[k, tp], rows.at[k, tp], core_send.at[k], core_recv.at[k], me, core)

    def forward(k):
        return remote(rows.at[k, cross], rows.at[k, cross], fwd_send.at[k], fwd_recv.at[k], me, core)

    def pair(k):
        return remote(part.at[k, 1 - b], pair_in.at[k], pair_send.at[k], pair_recv.at[k], me, core)

    def cross_sum(k):
        return remote(cross_out.at[k], cross_in.at[k], sum_send.at[k], sum_recv.at[k], me, cross)

    def give_back(k):
        return remote(result.at[k], back.at[k], ret_send.at[k], ret_recv.at[k], partner(k), tp)

    for copy in weights:
        copy.start()

    barrier = pltpu.get_barrier_semaphore()

    def greet(k, carry):
        pl.semaphore_signal(
            barrier, inc=1, device_id=(lax.rem(me + k, groups), tp), device_id_type=MESH
        )
        return carry

    lax.fori_loop(1, groups, greet, 0)
    pl.semaphore_signal(barrier, inc=1, device_id=(me, cross), device_id_type=MESH)
    pl.semaphore_signal(barrier, inc=1, device_id=(me, core), device_id_type=MESH)

    values = tokens[...].astype(jnp.float32)
    scale = lax.rsqrt(jnp.mean(values * values, axis=-1, keepdims=True) + NORM_EPS)

    def normed(index):
        span = pl.ds(pl.multiple_of(index * quarter, quarter), quarter)
        return (tokens[:, span].astype(jnp.float32) * scale * gain[:, span]).astype(jnp.bfloat16)

    normed_own[...] = normed(tp)
    normed_cross[...] = normed(cross)
    earlier = lax.broadcasted_iota(jnp.int32, (tok_count, tok_count), 0)
    later = lax.broadcasted_iota(jnp.int32, (tok_count, tok_count), 1)
    before[...] = jnp.where(earlier < later, 1.0, 0.0).astype(jnp.bfloat16)

    def select(k):
        expert = partner(k)
        hits = ids[...] == expert
        named = jnp.sum(jnp.where(hits, 1.0, 0.0), axis=0, keepdims=True)
        weight = jnp.sum(jnp.where(hits, route[...], 0.0), axis=0, keepdims=True)
        count = jnp.dot(
            jnp.broadcast_to(named, (8, tok_count)).astype(jnp.bfloat16),
            before[...],
            preferred_element_type=jnp.float32,
        )[0:1]
        slot = jnp.where(named > 0.0, count.astype(jnp.int32), -1)
        place = lax.broadcasted_iota(jnp.int32, (capacity, tok_count), 0)
        chosen = place == slot
        mix = jnp.where(chosen, weight, 0.0)
        mix_high = mix.astype(jnp.bfloat16)
        high[k] = mix_high
        low[k] = (mix - mix_high.astype(jnp.float32)).astype(jnp.bfloat16)
        return jnp.where(chosen, 1.0, 0.0).astype(jnp.bfloat16)

    def pick(chosen, source):
        return jnp.dot(chosen, source[...], preferred_element_type=jnp.float32).astype(jnp.bfloat16)

    chosen = select(0)
    rows[0, tp] = pick(chosen, normed_own)
    rows[0, cross] = pick(chosen, normed_cross)
    pl.semaphore_wait(barrier, groups + 1)

    def launch(i, carry):
        k = order(i)
        chosen = select(k)
        send[k] = pick(chosen, normed_own)
        dispatch(k).start()

        @pl.when(k < half)
        def _():
            send_cross[k] = pick(chosen, normed_cross)
            dispatch_cross(k).start()

        return carry

    lax.fori_loop(1, groups, launch, 0)
    for copy in weights:
        copy.wait()

    def step(i, carry):
        @pl.when(i >= 4)
        def _():
            k = order(i - 4)
            cross_sum(k).wait_recv()
            total = part[k, b, a].astype(jnp.float32) + pair_in[k, a].astype(jnp.float32)
            total = (total + cross_in[k].astype(jnp.float32)).astype(jnp.bfloat16)

            @pl.when(k == 0)
            def _():
                back[0] = total

            @pl.when(k > 0)
            def _():
                result[k] = total
                give_back(k).start()

        @pl.when((i >= 3) & (i < groups + 3))
        def _():
            k = order(i - 3)
            pair(k).wait_recv()
            total = part[k, b, 1 - a].astype(jnp.float32) + pair_in[k, 1 - a].astype(jnp.float32)
            cross_out[k] = total.astype(jnp.bfloat16)
            cross_sum(k).start()

        @pl.when((i >= 2) & (i < groups + 2))
        def _():
            k = order(i - 2)
            to_core(k).wait_recv()
            forward(k).wait_recv()
            block = jnp.concatenate([rows[k, j] for j in range(4)], axis=1)
            gate_sum = jnp.dot(block, gate_w[...], preferred_element_type=jnp.float32)
            up_sum = jnp.dot(block, up_w[...], preferred_element_type=jnp.float32)
            activated = activate(gate_sum, up_sum)
            for j in range(4):
                part[k, j % 2, j // 2] = jnp.dot(
                    activated,
                    down_w[:, j * quarter : (j + 1) * quarter],
                    preferred_element_type=jnp.float32,
                ).astype(jnp.bfloat16)
            pair(k).start()

        @pl.when((i >= 1) & (i < groups + 1))
        def _():
            k = order(i - 1)

            @pl.when(k > 0)
            def _():
                to_cross(k).wait_recv()

            forward(k).start()

        @pl.when(i < groups)
        def _():
            k = order(i)

            @pl.when(k > 0)
            def _():
                dispatch(k).wait_recv()

            @pl.when(k >= half)
            def _():
                to_cross(k).start()

            to_core(k).start()

        return carry

    lax.fori_loop(0, groups + 4, step, 0)

    total_out[...] = jnp.zeros_like(total_out)

    def finish(i, carry):
        k = order(i)

        @pl.when(k > 0)
        def _():
            give_back(k).wait_recv()

        for share in (high, low):
            total_out[...] += lax.dot_general(
                share[k], back[k], (((0,), (0,)), ((), ())), preferred_element_type=jnp.float32
            )
        return carry

    lax.fori_loop(0, groups, finish, 0)
    out[...] = total_out[...].astype(jnp.bfloat16)

    def drain(k, carry):
        to_core(k).wait_send()
        forward(k).wait_send()
        pair(k).wait_send()
        cross_sum(k).wait_send()

        @pl.when(k > 0)
        def _():
            to_cross(k).wait_send()
            dispatch(k).wait_send()
            give_back(k).wait_send()

        return carry

    lax.fori_loop(0, groups, drain, 0)


def shards(tokens, expert_ids, route_weight, norm_gain, expert_gate, expert_up, expert_down):
    groups = lax.axis_size("ep")
    tp_count = lax.axis_size("tp")
    experts = groups * expert_gate.shape[0]
    tok_count, model_width = tokens.shape
    top_count = expert_ids.shape[1]
    capacity = min(tok_count, 3 * tok_count * top_count // experts)
    quarter = model_width // tp_count
    bf16 = jnp.bfloat16
    slots = (groups, capacity, quarter)
    weights = (expert_gate[0], expert_up[0], expert_down[0])
    operands = (tokens, expert_ids.T, route_weight.T, norm_gain[None, :], *weights)
    if groups == 2 * PLANES and 2 * capacity > tok_count:
        return plane_call(groups, capacity, operands)
    return pl.pallas_call(
        functools.partial(expert_kernel, groups),
        out_shape=jax.ShapeDtypeStruct((tok_count, quarter), bf16),
        in_specs=[pl.BlockSpec(memory_space=pltpu.VMEM)] * 4
        + [pl.BlockSpec(memory_space=pl.ANY)] * 3,
        out_specs=pl.BlockSpec(memory_space=pltpu.VMEM),
        scratch_shapes=[
            *[pltpu.VMEM(weight.shape, bf16) for weight in weights],
            pltpu.VMEM((tok_count, quarter), bf16),
            pltpu.VMEM((tok_count, quarter), bf16),
            pltpu.VMEM((tok_count, tok_count), bf16),
            pltpu.VMEM(slots, bf16),
            pltpu.VMEM((groups // 2, capacity, quarter), bf16),
            pltpu.VMEM(slots, bf16),
            pltpu.VMEM((groups, capacity, tok_count), bf16),
            pltpu.VMEM((groups, capacity, tok_count), bf16),
            pltpu.VMEM((tok_count, quarter), jnp.float32),
            pltpu.VMEM((groups, 4, capacity, quarter), bf16),
            pltpu.VMEM((groups, 2, 2, capacity, quarter), bf16),
            pltpu.VMEM((groups, 2, capacity, quarter), bf16),
            pltpu.VMEM(slots, bf16),
            pltpu.VMEM(slots, bf16),
            pltpu.VMEM(slots, bf16),
            pltpu.SemaphoreType.DMA((3,)),
            *[pltpu.SemaphoreType.DMA((groups,)) for _ in range(14)],
        ],
        compiler_params=pltpu.CompilerParams(
            collective_id=0, has_side_effects=True, vmem_limit_bytes=60 * 1024 * 1024
        ),
    )(*operands)


def solution(mesh):
    return jax.shard_map(
        shards,
        mesh=mesh,
        in_specs=(
            P("ep", None),
            P("ep", None),
            P("ep", None),
            P(),
            P("ep", None, "tp"),
            P("ep", None, "tp"),
            P("ep", "tp", None),
        ),
        out_specs=P("ep", "tp"),
        check_vma=False,
    )
```

```python
import functools

import jax
import jax.numpy as jnp
from jax import lax
from jax.experimental import pallas as pl
from jax.experimental.pallas import tpu as pltpu
from jax.sharding import PartitionSpec as P

NORM_EPS = 1e-06
CLAMP_LIMIT = 7.0
SWISH_SCALE = 1.702
MESH = pl.DeviceIdType.MESH
STEPS = (
    "L13", "L33", "L32", "M0", "Y00", "A00", "F00", "G000", "G001", "B00",
    "L11", "L30", "M3", "Y33", "G003", "L31", "A33", "Y32", "A32", "G002",
    "M1", "A11", "B01", "L23", "L21", "L10", "B03", "A30", "Y30", "B33",
    "A13", "B02", "X303", "Y31", "B32", "L22", "A31", "Y13", "X302", "F01",
    "X300", "B30", "M2", "Y23", "B31", "A23", "G011", "G013", "H001", "Y11",
    "X301", "L12", "F30", "G010", "X313", "L20", "Y21", "X310", "X311", "B13",
    "X312", "A21", "B23", "H003", "A10", "Y10", "G300", "B11", "X203", "F31",
    "B21", "Y22", "H000", "A12", "G310", "Y12", "A22", "G312", "F10", "G313",
    "G311", "X211", "Y20", "H310", "B22", "B10", "H011", "B12", "G302", "H312",
    "G301", "X201", "F11", "A20", "H010", "B20", "H300", "H311", "X213", "X202",
    "G101", "X212", "H002", "G111", "G303", "S30", "F21", "H302", "G102", "G113",
    "S32", "H313", "G210", "G112", "H101", "H301", "S31", "G211", "H111", "F20",
    "G200", "G103", "H102", "G212", "H303", "H210", "G201", "G110", "G213", "S33",
    "S11", "G202", "H112", "H211", "H113", "H200", "S20", "S00", "J32", "H013",
    "G100", "G203", "S01", "H103", "S12", "H212", "H201", "S21", "H110", "J11",
    "J30", "J33", "G012", "J31", "S13", "S03", "H213", "H202", "S22", "H100",
    "S10", "J20", "H203", "S23", "J13", "H012", "J12", "S02", "J22", "J10",
    "J21", "J23",
)
CARRIED = ((2, 2, 2, 2), (2, 2, 2, 2), (2, 1, 1, 1), (1, 1, 1, 1))
PLANES, PARTS = len(CARRIED), len(CARRIED[0])


def activate(gate_sum, up_sum):
    gate_cut = jnp.minimum(gate_sum, CLAMP_LIMIT)
    up_cut = jnp.clip(up_sum, -CLAMP_LIMIT, CLAMP_LIMIT)
    return ((up_cut + 1.0) * gate_cut * jax.nn.sigmoid(SWISH_SCALE * gate_cut)).astype(jnp.bfloat16)


def plane_kernel(
    groups,
    tokens,
    ids,
    route,
    gain,
    gate_hbm,
    up_hbm,
    down_hbm,
    out,
    gate_w,
    up_w,
    down_w,
    token_in,
    id_in,
    route_in,
    gain_in,
    before,
    meta,
    normed,
    dense,
    picker,
    high,
    low,
    rows,
    picked,
    part,
    pair_in,
    cross_out,
    cross_in,
    result,
    plane_in,
    total,
    sum_out,
    sum_in,
    w_sem,
    io_sem,
    meta_send,
    meta_recv,
    dense_send,
    dense_recv,
    pick_send,
    pick_recv,
    core_send,
    core_recv,
    fwd_send,
    fwd_recv,
    pair_send,
    pair_recv,
    cross_send,
    cross_recv,
    near_send,
    near_recv,
    sum_send,
    sum_recv,
):
    me = lax.axis_index("ep")
    tp = lax.axis_index("tp")
    a, b = tp // 2, lax.rem(tp, 2)
    cross = 2 * (1 - a) + b
    core = 2 * a + 1 - b
    quarters = (tp, cross)
    slots, width = rows.shape[3:]
    quarter = PARTS * width
    tok_count = tokens.shape[0]
    f32, bf16 = jnp.float32, jnp.bfloat16
    moves = ((tokens, token_in), (gain, gain_in), (ids, id_in), (route, route_in))
    fetches = [pltpu.make_async_copy(*move, io_sem.at[i]) for i, move in enumerate(moves)]
    for fetch in fetches:
        fetch.start()

    def partner(k):
        total, bit = 0, 1
        while bit < groups:
            total += bit * lax.rem(me // bit + k // bit, 2)
            bit *= 2
        return total

    def remote(src, dst, send_sem, recv_sem, k, tp_index):
        return pltpu.make_async_remote_copy(
            src_ref=src,
            dst_ref=dst,
            send_sem=send_sem,
            recv_sem=recv_sem,
            device_id=(partner(k), tp_index),
            device_id_type=MESH,
        )

    def shares(d, h):
        return range(CARRIED[d][h])

    def settle(ref, sem):
        pltpu.make_async_copy(ref, ref, sem).wait()

    def describe(d):
        return remote(meta.at[0], meta.at[d], meta_send, meta_recv.at[d], 2 * d, tp)

    def spread(d, q, h):
        return remote(
            normed.at[quarters[q], h],
            dense.at[d - 1, q, h],
            dense_send.at[d, h],
            dense_recv.at[d, h],
            2 * d,
            tp,
        )

    def neighbour(d, q, h):
        return remote(
            picked.at[d, q, h],
            rows.at[2 * d + 1, quarters[q], h],
            pick_send.at[d, h],
            pick_recv.at[d, h],
            1,
            tp,
        )

    def to_core(k, q, h):
        ref = rows.at[k, quarters[q], h]
        return remote(ref, ref, core_send, core_recv.at[k], 0, core)

    def to_cross(k, h):
        ref = rows.at[k, tp, h]
        return remote(ref, ref, fwd_send, fwd_recv.at[k - PLANES, h], 0, cross)

    def pair(k, h):
        return remote(
            part.at[k, 1 - b, h], pair_in.at[k, h], pair_send, pair_recv.at[k, h], 0, core
        )

    def cross_sum(k, h):
        return remote(
            cross_out.at[k, h], cross_in.at[k, h], cross_send, cross_recv.at[k, h], 0, cross
        )

    def near_sum(d, h):
        return remote(
            result.at[2 * d + 1, h], plane_in.at[d, h], near_send, near_recv.at[d, h], 1, tp
        )

    def plane_sum(d, h):
        return remote(
            sum_out.at[d - 1, h], sum_in.at[d - 1, h], sum_send, sum_recv.at[d, h], 2 * d, tp
        )

    weights = [
        pltpu.make_async_copy(src, dst, w_sem.at[i])
        for i, (src, dst) in enumerate(((gate_hbm, gate_w), (up_hbm, up_w), (down_hbm, down_w)))
    ]
    barrier = pltpu.get_barrier_semaphore()
    peers = [(partner(2 * d), tp) for d in range(1, PLANES)]
    peers += [(partner(1), tp), (me, cross), (me, core)]
    for peer in peers:
        pl.semaphore_signal(barrier, inc=1, device_id=peer, device_id_type=MESH)

    for fetch in fetches:
        fetch.wait()
    for copy in weights:
        copy.start()
    values = token_in[...].astype(f32)
    scale = lax.rsqrt(jnp.mean(values * values, axis=-1, keepdims=True) + NORM_EPS)
    for j in range(4):
        for h in range(PARTS):
            span = slice(j * quarter + h * width, j * quarter + (h + 1) * width)
            normed[j, h] = (token_in[:, span].astype(f32) * scale * gain_in[:, span]).astype(bf16)
    meta[0, 0:2] = id_in[...].astype(f32)
    meta[0, 2:4] = route_in[...]
    pl.semaphore_wait(barrier, len(peers))
    for d in range(1, PLANES):
        describe(d).start()

    def L(d, h):
        for q in shares(d, h):
            spread(d, q, h).start()

    def M(d):
        if d:
            describe(d).wait_recv()
        else:
            earlier = lax.broadcasted_iota(jnp.int32, (tok_count, tok_count), 0)
            later = lax.broadcasted_iota(jnp.int32, (tok_count, tok_count), 1)
            before[...] = jnp.where(earlier < later, 1.0, 0.0).astype(bf16)
        for side in range(2):
            hits = meta[d, 0:2] == partner(side).astype(f32)
            named = jnp.sum(jnp.where(hits, 1.0, 0.0), axis=0, keepdims=True)
            weight = jnp.sum(jnp.where(hits, meta[d, 2:4], 0.0), axis=0, keepdims=True)
            count = jnp.dot(
                jnp.broadcast_to(named, (8, tok_count)).astype(bf16),
                before[...],
                preferred_element_type=f32,
            )[0:1]
            slot = jnp.where(named > 0.0, count.astype(jnp.int32), -1)
            place = lax.broadcasted_iota(jnp.int32, (slots, tok_count), 0)
            chosen = place == slot
            mix = jnp.where(chosen, weight, 0.0)
            mix_high = mix.astype(bf16)
            high[d, side] = mix_high
            low[d, side] = (mix - mix_high.astype(f32)).astype(bf16)
            picker[d, side] = jnp.where(chosen, 1.0, 0.0).astype(bf16)

    def block(d, q, h):
        return dense[d - 1, q, h] if d else normed[quarters[q], h]

    def pick(d, side, source):
        return jnp.dot(picker[d, side], source, preferred_element_type=f32).astype(bf16)

    arrived = set()

    def arrive(d, h):
        if d and (d, h) not in arrived:
            arrived.add((d, h))
            settle(dense.at[d - 1, 0 : CARRIED[d][h], h], dense_recv.at[d, h])

    def A(d, h):
        if d == 0:
            for j in range(4):
                for n in range(PARTS):
                    rows[0, j, n] = pick(0, 0, normed[j, n])
            return
        arrive(d, h)
        for q in shares(d, h):
            rows[2 * d, quarters[q], h] = pick(d, 0, block(d, q, h))
            to_core(2 * d, q, h).start()
        if len(shares(d, h)) == 1:
            to_cross(2 * d, h).start()

    def Y(d, h):
        arrive(d, h)
        for n in range(PARTS) if d == 0 else (h,):
            for q in shares(d, n):
                picked[d, q, n] = pick(d, 1, block(d, q, n))
                neighbour(d, q, n).start()

    def B(d, h):
        k = 2 * d + 1
        settle(picked.at[d, 0 : CARRIED[d][h], h], pick_recv.at[d, h])
        for q in shares(d, h):
            to_core(k, q, h).start()
        if len(shares(d, h)) == 1:
            to_cross(k, h).start()

    def X(d, side, h):
        k = 2 * d + side
        to_cross(k, h).wait_recv()
        to_core(k, 1, h).start()

    def F(d, side):
        k = 2 * d + side
        if (d, side) == FIRST:
            for copy in weights:
                copy.wait()
        if k:
            settle(rows.at[k, 0:2], core_recv.at[k])
        whole = jnp.concatenate([rows[k, j, h] for j in range(4) for h in range(PARTS)], axis=1)
        gate_sum = jnp.dot(whole, gate_w[...], preferred_element_type=f32)
        up_sum = jnp.dot(whole, up_w[...], preferred_element_type=f32)
        activated = activate(gate_sum, up_sum)
        for j in range(4):
            piece = jnp.dot(
                activated, down_w[:, j * quarter : (j + 1) * quarter], preferred_element_type=f32
            ).astype(bf16)
            for h in range(PARTS):
                part[k, j % 2, h, j // 2] = piece[:, h * width : (h + 1) * width]
        for h in range(PARTS):
            pair(k, h).start()

    def G(d, side, h):
        k = 2 * d + side
        pair(k, h).wait_recv()
        both = part[k, b, h, 1 - a].astype(f32) + pair_in[k, h, 1 - a].astype(f32)
        cross_out[k, h] = both.astype(bf16)
        cross_sum(k, h).start()

    def H(d, side, h):
        k = 2 * d + side
        cross_sum(k, h).wait_recv()
        both = part[k, b, h, a].astype(f32) + pair_in[k, h, a].astype(f32)
        result[k, h] = (both + cross_in[k, h].astype(f32)).astype(bf16)
        if side:
            near_sum(d, h).start()

    def S(d, h):
        near_sum(d, h).wait_recv()
        mixed = 0.0
        for side, value in ((0, result[2 * d, h]), (1, plane_in[d, h])):
            for share in (high, low):
                mixed += lax.dot_general(
                    share[d, side], value, (((0,), (0,)), ((), ())), preferred_element_type=f32
                )
        if d:
            sum_out[d - 1, h] = mixed.astype(bf16)
            plane_sum(d, h).start()
        else:
            total[h] = mixed

    def J(d, h):
        plane_sum(d, h).wait_recv()

    stages = dict(L=L, M=M, A=A, Y=Y, B=B, X=X, F=F, G=G, H=H, S=S, J=J)
    for step in STEPS:
        stages[step[0]](*(int(n) for n in step[1:]))

    for h in range(PARTS):
        mixed = total[h]
        for d in range(1, PLANES):
            mixed += sum_in[d - 1, h].astype(f32)
        out[:, h * width : (h + 1) * width] = mixed.astype(bf16)

    settle(meta.at[1:PLANES], meta_send)
    for d in range(PLANES):
        for h in range(PARTS):
            settle(picked.at[d, 0 : CARRIED[d][h], h], pick_send.at[d, h])
            if d:
                settle(dense.at[d - 1, 0 : CARRIED[d][h], h], dense_send.at[d, h])
    settle(rows.at[1:groups, 0:2], core_send)
    settle(rows.at[0 : sum(carry.count(1) for carry in CARRIED), 0, 0:2], fwd_send)
    settle(part.at[:, 0], pair_send)
    settle(cross_out, cross_send)
    settle(plane_in, near_send)
    settle(sum_out, sum_send)


FIRST = next((int(step[1]), int(step[2])) for step in STEPS if step[0] == "F")


def plane_call(groups, capacity, operands):
    tokens, weights = operands[0], operands[4:]
    tok_count, model_width = tokens.shape
    quarter = model_width // 4
    width = quarter // PARTS
    bf16, f32 = jnp.bfloat16, jnp.float32
    compact = (PARTS, capacity, width)
    full = (PARTS, tok_count, width)
    dma = pltpu.SemaphoreType.DMA
    return pl.pallas_call(
        functools.partial(plane_kernel, groups),
        out_shape=pltpu.VMEM((tok_count, quarter), bf16),
        in_specs=[pl.BlockSpec(memory_space=pl.ANY)] * len(operands),
        out_specs=pl.BlockSpec(memory_space=pltpu.VMEM),
        scratch_shapes=[
            *[pltpu.VMEM(weight.shape, bf16) for weight in weights],
            *[pltpu.VMEM(operands[n].shape, operands[n].dtype) for n in (0, 1, 2, 3)],
            pltpu.VMEM((tok_count, tok_count), bf16),
            pltpu.VMEM((PLANES, 8, tok_count), f32),
            pltpu.VMEM((4, *full), bf16),
            pltpu.VMEM((PLANES - 1, 2, *full), bf16),
            *[pltpu.VMEM((PLANES, 2, capacity, tok_count), bf16)] * 3,
            pltpu.VMEM((groups, 4, *compact), bf16),
            pltpu.VMEM((PLANES, 2, *compact), bf16),
            pltpu.VMEM((groups, 2, PARTS, 2, capacity, width), bf16),
            pltpu.VMEM((groups, PARTS, 2, capacity, width), bf16),
            *[pltpu.VMEM((groups, *compact), bf16)] * 3,
            pltpu.VMEM((PLANES, *compact), bf16),
            pltpu.VMEM(full, f32),
            *[pltpu.VMEM((PLANES - 1, *full), bf16)] * 2,
            dma((3,)),
            dma((4,)),
            dma,
            dma((PLANES,)),
            *[dma((PLANES, PARTS))] * 4,
            dma,
            dma((groups,)),
            dma,
            dma((groups - PLANES, PARTS)),
            dma,
            dma((groups, PARTS)),
            dma,
            dma((groups, PARTS)),
            dma,
            dma((PLANES, PARTS)),
            dma,
            dma((PLANES, PARTS)),
        ],
        compiler_params=pltpu.CompilerParams(
            collective_id=0, has_side_effects=True, vmem_limit_bytes=60 * 1024 * 1024
        ),
    )(*operands)


def expert_kernel(
    groups,
    tokens,
    ids,
    route,
    gain,
    gate_hbm,
    up_hbm,
    down_hbm,
    out,
    gate_w,
    up_w,
    down_w,
    normed_own,
    normed_cross,
    before,
    send,
    send_cross,
    back,
    high,
    low,
    total_out,
    rows,
    part,
    pair_in,
    cross_out,
    cross_in,
    result,
    w_sem,
    disp_send,
    disp_recv,
    cross_send,
    cross_recv,
    core_send,
    core_recv,
    fwd_send,
    fwd_recv,
    pair_send,
    pair_recv,
    sum_send,
    sum_recv,
    ret_send,
    ret_recv,
):
    me = lax.axis_index("ep")
    tp = lax.axis_index("tp")
    a, b = tp // 2, lax.rem(tp, 2)
    cross = 2 * (1 - a) + b
    core = 2 * a + 1 - b
    capacity, quarter = send.shape[1:]
    tok_count = tokens.shape[0]
    half = groups // 2

    weights = [
        pltpu.make_async_copy(src, dst, w_sem.at[i])
        for i, (src, dst) in enumerate(((gate_hbm, gate_w), (up_hbm, up_w), (down_hbm, down_w)))
    ]

    def remote(src, dst, send_sem, recv_sem, ep_index, tp_index):
        return pltpu.make_async_remote_copy(
            src_ref=src,
            dst_ref=dst,
            send_sem=send_sem,
            recv_sem=recv_sem,
            device_id=(ep_index, tp_index),
            device_id_type=MESH,
        )

    def partner(k):
        total, bit = 0, 1
        while bit < groups:
            total += bit * lax.rem(me // bit + k // bit, 2)
            bit *= 2
        return total

    def order(i):
        i = i + (i // (groups - 2)) * (1 - 2 * lax.rem(i, 2))
        return i // 2 + half * lax.rem(i, 2)

    def dispatch(k):
        dst = partner(k)
        return remote(send.at[k], rows.at[k, tp], disp_send.at[k], disp_recv.at[k], dst, tp)

    def dispatch_cross(k):
        dst = partner(k)
        return remote(
            send_cross.at[k],
            rows.at[k, cross],
            cross_send.at[k],
            cross_recv.at[k],
            dst,
            tp,
        )

    def to_cross(k):
        return remote(rows.at[k, tp], rows.at[k, tp], cross_send.at[k], cross_recv.at[k], me, cross)

    def to_core(k):
        return remote(rows.at[k, tp], rows.at[k, tp], core_send.at[k], core_recv.at[k], me, core)

    def forward(k):
        return remote(rows.at[k, cross], rows.at[k, cross], fwd_send.at[k], fwd_recv.at[k], me, core)

    def pair(k):
        return remote(part.at[k, 1 - b], pair_in.at[k], pair_send.at[k], pair_recv.at[k], me, core)

    def cross_sum(k):
        return remote(cross_out.at[k], cross_in.at[k], sum_send.at[k], sum_recv.at[k], me, cross)

    def give_back(k):
        return remote(result.at[k], back.at[k], ret_send.at[k], ret_recv.at[k], partner(k), tp)

    for copy in weights:
        copy.start()

    barrier = pltpu.get_barrier_semaphore()

    def greet(k, carry):
        pl.semaphore_signal(
            barrier, inc=1, device_id=(lax.rem(me + k, groups), tp), device_id_type=MESH
        )
        return carry

    lax.fori_loop(1, groups, greet, 0)
    pl.semaphore_signal(barrier, inc=1, device_id=(me, cross), device_id_type=MESH)
    pl.semaphore_signal(barrier, inc=1, device_id=(me, core), device_id_type=MESH)

    values = tokens[...].astype(jnp.float32)
    scale = lax.rsqrt(jnp.mean(values * values, axis=-1, keepdims=True) + NORM_EPS)

    def normed(index):
        span = pl.ds(pl.multiple_of(index * quarter, quarter), quarter)
        return (tokens[:, span].astype(jnp.float32) * scale * gain[:, span]).astype(jnp.bfloat16)

    normed_own[...] = normed(tp)
    normed_cross[...] = normed(cross)
    earlier = lax.broadcasted_iota(jnp.int32, (tok_count, tok_count), 0)
    later = lax.broadcasted_iota(jnp.int32, (tok_count, tok_count), 1)
    before[...] = jnp.where(earlier < later, 1.0, 0.0).astype(jnp.bfloat16)

    def select(k):
        expert = partner(k)
        hits = ids[...] == expert
        named = jnp.sum(jnp.where(hits, 1.0, 0.0), axis=0, keepdims=True)
        weight = jnp.sum(jnp.where(hits, route[...], 0.0), axis=0, keepdims=True)
        count = jnp.dot(
            jnp.broadcast_to(named, (8, tok_count)).astype(jnp.bfloat16),
            before[...],
            preferred_element_type=jnp.float32,
        )[0:1]
        slot = jnp.where(named > 0.0, count.astype(jnp.int32), -1)
        place = lax.broadcasted_iota(jnp.int32, (capacity, tok_count), 0)
        chosen = place == slot
        mix = jnp.where(chosen, weight, 0.0)
        mix_high = mix.astype(jnp.bfloat16)
        high[k] = mix_high
        low[k] = (mix - mix_high.astype(jnp.float32)).astype(jnp.bfloat16)
        return jnp.where(chosen, 1.0, 0.0).astype(jnp.bfloat16)

    def pick(chosen, source):
        return jnp.dot(chosen, source[...], preferred_element_type=jnp.float32).astype(jnp.bfloat16)

    chosen = select(0)
    rows[0, tp] = pick(chosen, normed_own)
    rows[0, cross] = pick(chosen, normed_cross)
    pl.semaphore_wait(barrier, groups + 1)

    def launch(i, carry):
        k = order(i)
        chosen = select(k)
        send[k] = pick(chosen, normed_own)
        dispatch(k).start()

        @pl.when(k < half)
        def _():
            send_cross[k] = pick(chosen, normed_cross)
            dispatch_cross(k).start()

        return carry

    lax.fori_loop(1, groups, launch, 0)
    for copy in weights:
        copy.wait()

    def step(i, carry):
        @pl.when(i >= 4)
        def _():
            k = order(i - 4)
            cross_sum(k).wait_recv()
            total = part[k, b, a].astype(jnp.float32) + pair_in[k, a].astype(jnp.float32)
            total = (total + cross_in[k].astype(jnp.float32)).astype(jnp.bfloat16)

            @pl.when(k == 0)
            def _():
                back[0] = total

            @pl.when(k > 0)
            def _():
                result[k] = total
                give_back(k).start()

        @pl.when((i >= 3) & (i < groups + 3))
        def _():
            k = order(i - 3)
            pair(k).wait_recv()
            total = part[k, b, 1 - a].astype(jnp.float32) + pair_in[k, 1 - a].astype(jnp.float32)
            cross_out[k] = total.astype(jnp.bfloat16)
            cross_sum(k).start()

        @pl.when((i >= 2) & (i < groups + 2))
        def _():
            k = order(i - 2)
            to_core(k).wait_recv()
            forward(k).wait_recv()
            block = jnp.concatenate([rows[k, j] for j in range(4)], axis=1)
            gate_sum = jnp.dot(block, gate_w[...], preferred_element_type=jnp.float32)
            up_sum = jnp.dot(block, up_w[...], preferred_element_type=jnp.float32)
            activated = activate(gate_sum, up_sum)
            for j in range(4):
                part[k, j % 2, j // 2] = jnp.dot(
                    activated,
                    down_w[:, j * quarter : (j + 1) * quarter],
                    preferred_element_type=jnp.float32,
                ).astype(jnp.bfloat16)
            pair(k).start()

        @pl.when((i >= 1) & (i < groups + 1))
        def _():
            k = order(i - 1)

            @pl.when(k > 0)
            def _():
                to_cross(k).wait_recv()

            forward(k).start()

        @pl.when(i < groups)
        def _():
            k = order(i)

            @pl.when(k > 0)
            def _():
                dispatch(k).wait_recv()

            @pl.when(k >= half)
            def _():
                to_cross(k).start()

            to_core(k).start()

        return carry

    lax.fori_loop(0, groups + 4, step, 0)

    total_out[...] = jnp.zeros_like(total_out)

    def finish(i, carry):
        k = order(i)

        @pl.when(k > 0)
        def _():
            give_back(k).wait_recv()

        for share in (high, low):
            total_out[...] += lax.dot_general(
                share[k], back[k], (((0,), (0,)), ((), ())), preferred_element_type=jnp.float32
            )
        return carry

    lax.fori_loop(0, groups, finish, 0)
    out[...] = total_out[...].astype(jnp.bfloat16)

    def drain(k, carry):
        to_core(k).wait_send()
        forward(k).wait_send()
        pair(k).wait_send()
        cross_sum(k).wait_send()

        @pl.when(k > 0)
        def _():
            to_cross(k).wait_send()
            dispatch(k).wait_send()
            give_back(k).wait_send()

        return carry

    lax.fori_loop(0, groups, drain, 0)


def shards(tokens, expert_ids, route_weight, norm_gain, expert_gate, expert_up, expert_down):
    groups = lax.axis_size("ep")
    tp_count = lax.axis_size("tp")
    experts = groups * expert_gate.shape[0]
    tok_count, model_width = tokens.shape
    top_count = expert_ids.shape[1]
    capacity = min(tok_count, 3 * tok_count * top_count // experts)
    quarter = model_width // tp_count
    bf16 = jnp.bfloat16
    slots = (groups, capacity, quarter)
    weights = (expert_gate[0], expert_up[0], expert_down[0])
    operands = (tokens, expert_ids.T, route_weight.T, norm_gain[None, :], *weights)
    if groups == 2 * PLANES and 2 * capacity > tok_count:
        return plane_call(groups, capacity, operands)
    return pl.pallas_call(
        functools.partial(expert_kernel, groups),
        out_shape=jax.ShapeDtypeStruct((tok_count, quarter), bf16),
        in_specs=[pl.BlockSpec(memory_space=pltpu.VMEM)] * 4
        + [pl.BlockSpec(memory_space=pl.ANY)] * 3,
        out_specs=pl.BlockSpec(memory_space=pltpu.VMEM),
        scratch_shapes=[
            *[pltpu.VMEM(weight.shape, bf16) for weight in weights],
            pltpu.VMEM((tok_count, quarter), bf16),
            pltpu.VMEM((tok_count, quarter), bf16),
            pltpu.VMEM((tok_count, tok_count), bf16),
            pltpu.VMEM(slots, bf16),
            pltpu.VMEM((groups // 2, capacity, quarter), bf16),
            pltpu.VMEM(slots, bf16),
            pltpu.VMEM((groups, capacity, tok_count), bf16),
            pltpu.VMEM((groups, capacity, tok_count), bf16),
            pltpu.VMEM((tok_count, quarter), jnp.float32),
            pltpu.VMEM((groups, 4, capacity, quarter), bf16),
            pltpu.VMEM((groups, 2, 2, capacity, quarter), bf16),
            pltpu.VMEM((groups, 2, capacity, quarter), bf16),
            pltpu.VMEM(slots, bf16),
            pltpu.VMEM(slots, bf16),
            pltpu.VMEM(slots, bf16),
            pltpu.SemaphoreType.DMA((3,)),
            *[pltpu.SemaphoreType.DMA((groups,)) for _ in range(14)],
        ],
        compiler_params=pltpu.CompilerParams(
            collective_id=0, has_side_effects=True, vmem_limit_bytes=60 * 1024 * 1024
        ),
    )(*operands)


def solution(mesh):
    return jax.shard_map(
        shards,
        mesh=mesh,
        in_specs=(
            P("ep", None),
            P("ep", None),
            P("ep", None),
            P(),
            P("ep", None, "tp"),
            P("ep", None, "tp"),
            P("ep", "tp", None),
        ),
        out_specs=P("ep", "tp"),
        check_vma=False,
    )
```

```python
import functools

import jax
import jax.numpy as jnp
from jax import lax
from jax.experimental import pallas as pl
from jax.experimental.pallas import tpu as pltpu
from jax.sharding import PartitionSpec as P

NORM_EPS = 1e-06
CLAMP_LIMIT = 7.0
SWISH_SCALE = 1.702
MESH = pl.DeviceIdType.MESH
STEPS = (
    "L13", "L33", "L32", "M0", "Y00", "A00", "F00", "G001", "B00", "G000",
    "L11", "L30", "M3", "Y33", "G003", "L31", "A33", "Y32", "A32", "G002",
    "M1", "A11", "B01", "L23", "L21", "L10", "B03", "A30", "Y30", "B33",
    "A13", "B02", "X303", "Y31", "B32", "L22", "A31", "Y13", "X302", "F01",
    "X300", "B30", "M2", "Y23", "B31", "A23", "G011", "G013", "H001", "Y11",
    "X301", "L12", "F30", "G010", "X313", "L20", "Y21", "A21", "B13", "X310",
    "X311", "X312", "H003", "A10", "B23", "Y10", "G300", "B11", "X203", "F31",
    "B21", "Y22", "H000", "A12", "G310", "Y12", "A22", "G312", "F10", "G313",
    "G311", "X211", "Y20", "H310", "B22", "B10", "H011", "B12", "G302", "H312",
    "G301", "X201", "F11", "A20", "H010", "B20", "H300", "H311", "X213", "X202",
    "G101", "X212", "H002", "G111", "G303", "S30", "F21", "H302", "G102", "G113",
    "S32", "H313", "G210", "G112", "H101", "H301", "S31", "G211", "H111", "F20",
    "G200", "G103", "H102", "G212", "H303", "H210", "G201", "G110", "G213", "S33",
    "S11", "G202", "H112", "H211", "H113", "H200", "S20", "S00", "J32", "H013",
    "G100", "G203", "S01", "H103", "S12", "H212", "H201", "S21", "J30", "H110",
    "J11", "J33", "G012", "J31", "S13", "S03", "H213", "H202", "S22", "H100",
    "S10", "J20", "H203", "S23", "J13", "H012", "J12", "S02", "J22", "J10",
    "J21", "J23",
)
CARRIED = ((2, 2, 2, 2), (2, 2, 2, 2), (2, 1, 1, 1), (1, 1, 1, 1))
PLANES, PARTS = len(CARRIED), len(CARRIED[0])


def activate(gate_sum, up_sum):
    gate_cut = jnp.minimum(gate_sum, CLAMP_LIMIT)
    up_cut = jnp.clip(up_sum, -CLAMP_LIMIT, CLAMP_LIMIT)
    return ((up_cut + 1.0) * gate_cut * jax.nn.sigmoid(SWISH_SCALE * gate_cut)).astype(jnp.bfloat16)


def plane_kernel(
    groups,
    tokens,
    ids,
    route,
    gain,
    gate_hbm,
    up_hbm,
    down_hbm,
    out,
    gate_w,
    up_w,
    down_w,
    token_in,
    id_in,
    route_in,
    gain_in,
    before,
    meta,
    normed,
    dense,
    picker,
    high,
    low,
    rows,
    picked,
    part,
    pair_in,
    cross_out,
    cross_in,
    result,
    plane_in,
    total,
    sum_out,
    sum_in,
    w_sem,
    io_sem,
    meta_send,
    meta_recv,
    dense_send,
    dense_recv,
    pick_send,
    pick_recv,
    core_send,
    core_recv,
    fwd_send,
    fwd_recv,
    pair_send,
    pair_recv,
    cross_send,
    cross_recv,
    near_send,
    near_recv,
    sum_send,
    sum_recv,
):
    me = lax.axis_index("ep")
    tp = lax.axis_index("tp")
    a, b = tp // 2, lax.rem(tp, 2)
    cross = 2 * (1 - a) + b
    core = 2 * a + 1 - b
    quarters = (tp, cross)
    slots, width = rows.shape[3:]
    quarter = PARTS * width
    tok_count = tokens.shape[0]
    f32, bf16 = jnp.float32, jnp.bfloat16
    moves = ((tokens, token_in), (gain, gain_in), (ids, id_in), (route, route_in))
    fetches = [pltpu.make_async_copy(*move, io_sem.at[i]) for i, move in enumerate(moves)]
    for fetch in fetches:
        fetch.start()

    def partner(k):
        total, bit = 0, 1
        while bit < groups:
            total += bit * lax.rem(me // bit + k // bit, 2)
            bit *= 2
        return total

    def remote(src, dst, send_sem, recv_sem, k, tp_index):
        return pltpu.make_async_remote_copy(
            src_ref=src,
            dst_ref=dst,
            send_sem=send_sem,
            recv_sem=recv_sem,
            device_id=(partner(k), tp_index),
            device_id_type=MESH,
        )

    def shares(d, h):
        return range(CARRIED[d][h])

    def settle(ref, sem):
        pltpu.make_async_copy(ref, ref, sem).wait()

    def describe(d):
        return remote(meta.at[0], meta.at[d], meta_send, meta_recv.at[d], 2 * d, tp)

    def spread(d, q, h):
        return remote(
            normed.at[quarters[q], h],
            dense.at[d - 1, q, h],
            dense_send.at[d, h],
            dense_recv.at[d, h],
            2 * d,
            tp,
        )

    def neighbour(d, q, h):
        return remote(
            picked.at[d, q, h],
            rows.at[2 * d + 1, quarters[q], h],
            pick_send.at[d, h],
            pick_recv.at[d, h],
            1,
            tp,
        )

    def to_core(k, q, h):
        ref = rows.at[k, quarters[q], h]
        return remote(ref, ref, core_send, core_recv.at[k], 0, core)

    def to_cross(k, h):
        ref = rows.at[k, tp, h]
        return remote(ref, ref, fwd_send, fwd_recv.at[k - PLANES, h], 0, cross)

    def pair(k, h):
        return remote(
            part.at[k, 1 - b, h], pair_in.at[k, h], pair_send, pair_recv.at[k, h], 0, core
        )

    def cross_sum(k, h):
        return remote(
            cross_out.at[k, h], cross_in.at[k, h], cross_send, cross_recv.at[k, h], 0, cross
        )

    def near_sum(d, h):
        return remote(
            result.at[2 * d + 1, h], plane_in.at[d, h], near_send, near_recv.at[d, h], 1, tp
        )

    def plane_sum(d, h):
        return remote(
            sum_out.at[d - 1, h], sum_in.at[d - 1, h], sum_send, sum_recv.at[d, h], 2 * d, tp
        )

    weights = [
        pltpu.make_async_copy(src, dst, w_sem.at[i])
        for i, (src, dst) in enumerate(((gate_hbm, gate_w), (up_hbm, up_w), (down_hbm, down_w)))
    ]
    barrier = pltpu.get_barrier_semaphore()
    peers = [(partner(2 * d), tp) for d in range(1, PLANES)]
    peers += [(partner(1), tp), (me, cross), (me, core)]
    for peer in peers:
        pl.semaphore_signal(barrier, inc=1, device_id=peer, device_id_type=MESH)

    for fetch in fetches:
        fetch.wait()
    for copy in weights:
        copy.start()
    values = token_in[...].astype(f32)
    scale = lax.rsqrt(jnp.mean(values * values, axis=-1, keepdims=True) + NORM_EPS)
    for j in range(4):
        for h in range(PARTS):
            span = slice(j * quarter + h * width, j * quarter + (h + 1) * width)
            normed[j, h] = (token_in[:, span].astype(f32) * scale * gain_in[:, span]).astype(bf16)
    meta[0, 0:2] = id_in[...].astype(f32)
    meta[0, 2:4] = route_in[...]
    pl.semaphore_wait(barrier, len(peers))
    for d in range(1, PLANES):
        describe(d).start()

    def L(d, h):
        for q in shares(d, h):
            spread(d, q, h).start()

    def M(d):
        if d:
            describe(d).wait_recv()
        else:
            earlier = lax.broadcasted_iota(jnp.int32, (tok_count, tok_count), 0)
            later = lax.broadcasted_iota(jnp.int32, (tok_count, tok_count), 1)
            before[...] = jnp.where(earlier < later, 1.0, 0.0).astype(bf16)
        for side in range(2):
            hits = meta[d, 0:2] == partner(side).astype(f32)
            named = jnp.sum(jnp.where(hits, 1.0, 0.0), axis=0, keepdims=True)
            weight = jnp.sum(jnp.where(hits, meta[d, 2:4], 0.0), axis=0, keepdims=True)
            count = jnp.dot(
                jnp.broadcast_to(named, (8, tok_count)).astype(bf16),
                before[...],
                preferred_element_type=f32,
            )[0:1]
            slot = jnp.where(named > 0.0, count.astype(jnp.int32), -1)
            place = lax.broadcasted_iota(jnp.int32, (slots, tok_count), 0)
            chosen = place == slot
            mix = jnp.where(chosen, weight, 0.0)
            mix_high = mix.astype(bf16)
            high[d, side] = mix_high
            low[d, side] = (mix - mix_high.astype(f32)).astype(bf16)
            picker[d, side] = jnp.where(chosen, 1.0, 0.0).astype(bf16)

    def block(d, q, h):
        return dense[d - 1, q, h] if d else normed[quarters[q], h]

    def pick(d, side, source):
        return jnp.dot(picker[d, side], source, preferred_element_type=f32).astype(bf16)

    arrived = set()

    def arrive(d, h):
        if d and (d, h) not in arrived:
            arrived.add((d, h))
            settle(dense.at[d - 1, 0 : CARRIED[d][h], h], dense_recv.at[d, h])

    def A(d, h):
        if d == 0:
            for j in range(4):
                for n in range(PARTS):
                    rows[0, j, n] = pick(0, 0, normed[j, n])
            return
        arrive(d, h)
        for q in shares(d, h):
            rows[2 * d, quarters[q], h] = pick(d, 0, block(d, q, h))
            to_core(2 * d, q, h).start()
        if len(shares(d, h)) == 1:
            to_cross(2 * d, h).start()

    def Y(d, h):
        arrive(d, h)
        for n in range(PARTS) if d == 0 else (h,):
            for q in shares(d, n):
                picked[d, q, n] = pick(d, 1, block(d, q, n))
                neighbour(d, q, n).start()

    def B(d, h):
        k = 2 * d + 1
        settle(picked.at[d, 0 : CARRIED[d][h], h], pick_recv.at[d, h])
        for q in shares(d, h):
            to_core(k, q, h).start()
        if len(shares(d, h)) == 1:
            to_cross(k, h).start()

    def X(d, side, h):
        k = 2 * d + side
        to_cross(k, h).wait_recv()
        to_core(k, 1, h).start()

    def F(d, side):
        k = 2 * d + side
        if (d, side) == FIRST:
            for copy in weights:
                copy.wait()
        if k:
            settle(rows.at[k, 0:2], core_recv.at[k])
        whole = jnp.concatenate([rows[k, j, h] for j in range(4) for h in range(PARTS)], axis=1)
        gate_sum = jnp.dot(whole, gate_w[...], preferred_element_type=f32)
        up_sum = jnp.dot(whole, up_w[...], preferred_element_type=f32)
        activated = activate(gate_sum, up_sum)
        for j in range(4):
            piece = jnp.dot(
                activated, down_w[:, j * quarter : (j + 1) * quarter], preferred_element_type=f32
            ).astype(bf16)
            for h in range(PARTS):
                part[k, j % 2, h, j // 2] = piece[:, h * width : (h + 1) * width]
        for h in range(PARTS):
            pair(k, h).start()

    def G(d, side, h):
        k = 2 * d + side
        pair(k, h).wait_recv()
        both = part[k, b, h, 1 - a].astype(f32) + pair_in[k, h, 1 - a].astype(f32)
        cross_out[k, h] = both.astype(bf16)
        cross_sum(k, h).start()

    def H(d, side, h):
        k = 2 * d + side
        cross_sum(k, h).wait_recv()
        both = part[k, b, h, a].astype(f32) + pair_in[k, h, a].astype(f32)
        result[k, h] = (both + cross_in[k, h].astype(f32)).astype(bf16)
        if side:
            near_sum(d, h).start()

    def S(d, h):
        near_sum(d, h).wait_recv()
        mixed = 0.0
        for side, value in ((0, result[2 * d, h]), (1, plane_in[d, h])):
            for share in (high, low):
                mixed += lax.dot_general(
                    share[d, side], value, (((0,), (0,)), ((), ())), preferred_element_type=f32
                )
        if d:
            sum_out[d - 1, h] = mixed.astype(bf16)
            plane_sum(d, h).start()
        else:
            total[h] = mixed

    def J(d, h):
        plane_sum(d, h).wait_recv()

    stages = dict(L=L, M=M, A=A, Y=Y, B=B, X=X, F=F, G=G, H=H, S=S, J=J)
    for step in STEPS:
        stages[step[0]](*(int(n) for n in step[1:]))

    for h in range(PARTS):
        mixed = total[h]
        for d in range(1, PLANES):
            mixed += sum_in[d - 1, h].astype(f32)
        out[:, h * width : (h + 1) * width] = mixed.astype(bf16)

    settle(meta.at[1:PLANES], meta_send)
    for d in range(PLANES):
        for h in range(PARTS):
            settle(picked.at[d, 0 : CARRIED[d][h], h], pick_send.at[d, h])
            if d:
                settle(dense.at[d - 1, 0 : CARRIED[d][h], h], dense_send.at[d, h])
    settle(rows.at[1:groups, 0:2], core_send)
    settle(rows.at[0 : sum(carry.count(1) for carry in CARRIED), 0, 0:2], fwd_send)
    settle(part.at[:, 0], pair_send)
    settle(cross_out, cross_send)
    settle(plane_in, near_send)
    settle(sum_out, sum_send)


FIRST = next((int(step[1]), int(step[2])) for step in STEPS if step[0] == "F")


def plane_call(groups, capacity, operands):
    tokens, weights = operands[0], operands[4:]
    tok_count, model_width = tokens.shape
    quarter = model_width // 4
    width = quarter // PARTS
    bf16, f32 = jnp.bfloat16, jnp.float32
    compact = (PARTS, capacity, width)
    full = (PARTS, tok_count, width)
    dma = pltpu.SemaphoreType.DMA
    return pl.pallas_call(
        functools.partial(plane_kernel, groups),
        out_shape=pltpu.VMEM((tok_count, quarter), bf16),
        in_specs=[pl.BlockSpec(memory_space=pl.ANY)] * len(operands),
        out_specs=pl.BlockSpec(memory_space=pltpu.VMEM),
        scratch_shapes=[
            *[pltpu.VMEM(weight.shape, bf16) for weight in weights],
            *[pltpu.VMEM(operands[n].shape, operands[n].dtype) for n in (0, 1, 2, 3)],
            pltpu.VMEM((tok_count, tok_count), bf16),
            pltpu.VMEM((PLANES, 8, tok_count), f32),
            pltpu.VMEM((4, *full), bf16),
            pltpu.VMEM((PLANES - 1, 2, *full), bf16),
            *[pltpu.VMEM((PLANES, 2, capacity, tok_count), bf16)] * 3,
            pltpu.VMEM((groups, 4, *compact), bf16),
            pltpu.VMEM((PLANES, 2, *compact), bf16),
            pltpu.VMEM((groups, 2, PARTS, 2, capacity, width), bf16),
            pltpu.VMEM((groups, PARTS, 2, capacity, width), bf16),
            *[pltpu.VMEM((groups, *compact), bf16)] * 3,
            pltpu.VMEM((PLANES, *compact), bf16),
            pltpu.VMEM(full, f32),
            *[pltpu.VMEM((PLANES - 1, *full), bf16)] * 2,
            dma((3,)),
            dma((4,)),
            dma,
            dma((PLANES,)),
            *[dma((PLANES, PARTS))] * 4,
            dma,
            dma((groups,)),
            dma,
            dma((groups - PLANES, PARTS)),
            dma,
            dma((groups, PARTS)),
            dma,
            dma((groups, PARTS)),
            dma,
            dma((PLANES, PARTS)),
            dma,
            dma((PLANES, PARTS)),
        ],
        compiler_params=pltpu.CompilerParams(
            collective_id=0, has_side_effects=True, vmem_limit_bytes=60 * 1024 * 1024
        ),
    )(*operands)


def expert_kernel(
    groups,
    tokens,
    ids,
    route,
    gain,
    gate_hbm,
    up_hbm,
    down_hbm,
    out,
    gate_w,
    up_w,
    down_w,
    normed_own,
    normed_cross,
    before,
    send,
    send_cross,
    back,
    high,
    low,
    total_out,
    rows,
    part,
    pair_in,
    cross_out,
    cross_in,
    result,
    w_sem,
    disp_send,
    disp_recv,
    cross_send,
    cross_recv,
    core_send,
    core_recv,
    fwd_send,
    fwd_recv,
    pair_send,
    pair_recv,
    sum_send,
    sum_recv,
    ret_send,
    ret_recv,
):
    me = lax.axis_index("ep")
    tp = lax.axis_index("tp")
    a, b = tp // 2, lax.rem(tp, 2)
    cross = 2 * (1 - a) + b
    core = 2 * a + 1 - b
    capacity, quarter = send.shape[1:]
    tok_count = tokens.shape[0]
    half = groups // 2

    weights = [
        pltpu.make_async_copy(src, dst, w_sem.at[i])
        for i, (src, dst) in enumerate(((gate_hbm, gate_w), (up_hbm, up_w), (down_hbm, down_w)))
    ]

    def remote(src, dst, send_sem, recv_sem, ep_index, tp_index):
        return pltpu.make_async_remote_copy(
            src_ref=src,
            dst_ref=dst,
            send_sem=send_sem,
            recv_sem=recv_sem,
            device_id=(ep_index, tp_index),
            device_id_type=MESH,
        )

    def partner(k):
        total, bit = 0, 1
        while bit < groups:
            total += bit * lax.rem(me // bit + k // bit, 2)
            bit *= 2
        return total

    def order(i):
        i = i + (i // (groups - 2)) * (1 - 2 * lax.rem(i, 2))
        return i // 2 + half * lax.rem(i, 2)

    def dispatch(k):
        dst = partner(k)
        return remote(send.at[k], rows.at[k, tp], disp_send.at[k], disp_recv.at[k], dst, tp)

    def dispatch_cross(k):
        dst = partner(k)
        return remote(
            send_cross.at[k],
            rows.at[k, cross],
            cross_send.at[k],
            cross_recv.at[k],
            dst,
            tp,
        )

    def to_cross(k):
        return remote(rows.at[k, tp], rows.at[k, tp], cross_send.at[k], cross_recv.at[k], me, cross)

    def to_core(k):
        return remote(rows.at[k, tp], rows.at[k, tp], core_send.at[k], core_recv.at[k], me, core)

    def forward(k):
        return remote(rows.at[k, cross], rows.at[k, cross], fwd_send.at[k], fwd_recv.at[k], me, core)

    def pair(k):
        return remote(part.at[k, 1 - b], pair_in.at[k], pair_send.at[k], pair_recv.at[k], me, core)

    def cross_sum(k):
        return remote(cross_out.at[k], cross_in.at[k], sum_send.at[k], sum_recv.at[k], me, cross)

    def give_back(k):
        return remote(result.at[k], back.at[k], ret_send.at[k], ret_recv.at[k], partner(k), tp)

    for copy in weights:
        copy.start()

    barrier = pltpu.get_barrier_semaphore()

    def greet(k, carry):
        pl.semaphore_signal(
            barrier, inc=1, device_id=(lax.rem(me + k, groups), tp), device_id_type=MESH
        )
        return carry

    lax.fori_loop(1, groups, greet, 0)
    pl.semaphore_signal(barrier, inc=1, device_id=(me, cross), device_id_type=MESH)
    pl.semaphore_signal(barrier, inc=1, device_id=(me, core), device_id_type=MESH)

    values = tokens[...].astype(jnp.float32)
    scale = lax.rsqrt(jnp.mean(values * values, axis=-1, keepdims=True) + NORM_EPS)

    def normed(index):
        span = pl.ds(pl.multiple_of(index * quarter, quarter), quarter)
        return (tokens[:, span].astype(jnp.float32) * scale * gain[:, span]).astype(jnp.bfloat16)

    normed_own[...] = normed(tp)
    normed_cross[...] = normed(cross)
    earlier = lax.broadcasted_iota(jnp.int32, (tok_count, tok_count), 0)
    later = lax.broadcasted_iota(jnp.int32, (tok_count, tok_count), 1)
    before[...] = jnp.where(earlier < later, 1.0, 0.0).astype(jnp.bfloat16)

    def select(k):
        expert = partner(k)
        hits = ids[...] == expert
        named = jnp.sum(jnp.where(hits, 1.0, 0.0), axis=0, keepdims=True)
        weight = jnp.sum(jnp.where(hits, route[...], 0.0), axis=0, keepdims=True)
        count = jnp.dot(
            jnp.broadcast_to(named, (8, tok_count)).astype(jnp.bfloat16),
            before[...],
            preferred_element_type=jnp.float32,
        )[0:1]
        slot = jnp.where(named > 0.0, count.astype(jnp.int32), -1)
        place = lax.broadcasted_iota(jnp.int32, (capacity, tok_count), 0)
        chosen = place == slot
        mix = jnp.where(chosen, weight, 0.0)
        mix_high = mix.astype(jnp.bfloat16)
        high[k] = mix_high
        low[k] = (mix - mix_high.astype(jnp.float32)).astype(jnp.bfloat16)
        return jnp.where(chosen, 1.0, 0.0).astype(jnp.bfloat16)

    def pick(chosen, source):
        return jnp.dot(chosen, source[...], preferred_element_type=jnp.float32).astype(jnp.bfloat16)

    chosen = select(0)
    rows[0, tp] = pick(chosen, normed_own)
    rows[0, cross] = pick(chosen, normed_cross)
    pl.semaphore_wait(barrier, groups + 1)

    def launch(i, carry):
        k = order(i)
        chosen = select(k)
        send[k] = pick(chosen, normed_own)
        dispatch(k).start()

        @pl.when(k < half)
        def _():
            send_cross[k] = pick(chosen, normed_cross)
            dispatch_cross(k).start()

        return carry

    lax.fori_loop(1, groups, launch, 0)
    for copy in weights:
        copy.wait()

    def step(i, carry):
        @pl.when(i >= 4)
        def _():
            k = order(i - 4)
            cross_sum(k).wait_recv()
            total = part[k, b, a].astype(jnp.float32) + pair_in[k, a].astype(jnp.float32)
            total = (total + cross_in[k].astype(jnp.float32)).astype(jnp.bfloat16)

            @pl.when(k == 0)
            def _():
                back[0] = total

            @pl.when(k > 0)
            def _():
                result[k] = total
                give_back(k).start()

        @pl.when((i >= 3) & (i < groups + 3))
        def _():
            k = order(i - 3)
            pair(k).wait_recv()
            total = part[k, b, 1 - a].astype(jnp.float32) + pair_in[k, 1 - a].astype(jnp.float32)
            cross_out[k] = total.astype(jnp.bfloat16)
            cross_sum(k).start()

        @pl.when((i >= 2) & (i < groups + 2))
        def _():
            k = order(i - 2)
            to_core(k).wait_recv()
            forward(k).wait_recv()
            block = jnp.concatenate([rows[k, j] for j in range(4)], axis=1)
            gate_sum = jnp.dot(block, gate_w[...], preferred_element_type=jnp.float32)
            up_sum = jnp.dot(block, up_w[...], preferred_element_type=jnp.float32)
            activated = activate(gate_sum, up_sum)
            for j in range(4):
                part[k, j % 2, j // 2] = jnp.dot(
                    activated,
                    down_w[:, j * quarter : (j + 1) * quarter],
                    preferred_element_type=jnp.float32,
                ).astype(jnp.bfloat16)
            pair(k).start()

        @pl.when((i >= 1) & (i < groups + 1))
        def _():
            k = order(i - 1)

            @pl.when(k > 0)
            def _():
                to_cross(k).wait_recv()

            forward(k).start()

        @pl.when(i < groups)
        def _():
            k = order(i)

            @pl.when(k > 0)
            def _():
                dispatch(k).wait_recv()

            @pl.when(k >= half)
            def _():
                to_cross(k).start()

            to_core(k).start()

        return carry

    lax.fori_loop(0, groups + 4, step, 0)

    total_out[...] = jnp.zeros_like(total_out)

    def finish(i, carry):
        k = order(i)

        @pl.when(k > 0)
        def _():
            give_back(k).wait_recv()

        for share in (high, low):
            total_out[...] += lax.dot_general(
                share[k], back[k], (((0,), (0,)), ((), ())), preferred_element_type=jnp.float32
            )
        return carry

    lax.fori_loop(0, groups, finish, 0)
    out[...] = total_out[...].astype(jnp.bfloat16)

    def drain(k, carry):
        to_core(k).wait_send()
        forward(k).wait_send()
        pair(k).wait_send()
        cross_sum(k).wait_send()

        @pl.when(k > 0)
        def _():
            to_cross(k).wait_send()
            dispatch(k).wait_send()
            give_back(k).wait_send()

        return carry

    lax.fori_loop(0, groups, drain, 0)


def shards(tokens, expert_ids, route_weight, norm_gain, expert_gate, expert_up, expert_down):
    groups = lax.axis_size("ep")
    tp_count = lax.axis_size("tp")
    experts = groups * expert_gate.shape[0]
    tok_count, model_width = tokens.shape
    top_count = expert_ids.shape[1]
    capacity = min(tok_count, 3 * tok_count * top_count // experts)
    quarter = model_width // tp_count
    bf16 = jnp.bfloat16
    slots = (groups, capacity, quarter)
    weights = (expert_gate[0], expert_up[0], expert_down[0])
    operands = (tokens, expert_ids.T, route_weight.T, norm_gain[None, :], *weights)
    if groups == 2 * PLANES and 2 * capacity > tok_count:
        return plane_call(groups, capacity, operands)
    return pl.pallas_call(
        functools.partial(expert_kernel, groups),
        out_shape=jax.ShapeDtypeStruct((tok_count, quarter), bf16),
        in_specs=[pl.BlockSpec(memory_space=pltpu.VMEM)] * 4
        + [pl.BlockSpec(memory_space=pl.ANY)] * 3,
        out_specs=pl.BlockSpec(memory_space=pltpu.VMEM),
        scratch_shapes=[
            *[pltpu.VMEM(weight.shape, bf16) for weight in weights],
            pltpu.VMEM((tok_count, quarter), bf16),
            pltpu.VMEM((tok_count, quarter), bf16),
            pltpu.VMEM((tok_count, tok_count), bf16),
            pltpu.VMEM(slots, bf16),
            pltpu.VMEM((groups // 2, capacity, quarter), bf16),
            pltpu.VMEM(slots, bf16),
            pltpu.VMEM((groups, capacity, tok_count), bf16),
            pltpu.VMEM((groups, capacity, tok_count), bf16),
            pltpu.VMEM((tok_count, quarter), jnp.float32),
            pltpu.VMEM((groups, 4, capacity, quarter), bf16),
            pltpu.VMEM((groups, 2, 2, capacity, quarter), bf16),
            pltpu.VMEM((groups, 2, capacity, quarter), bf16),
            pltpu.VMEM(slots, bf16),
            pltpu.VMEM(slots, bf16),
            pltpu.VMEM(slots, bf16),
            pltpu.SemaphoreType.DMA((3,)),
            *[pltpu.SemaphoreType.DMA((groups,)) for _ in range(14)],
        ],
        compiler_params=pltpu.CompilerParams(
            collective_id=0, has_side_effects=True, vmem_limit_bytes=60 * 1024 * 1024
        ),
    )(*operands)


def solution(mesh):
    return jax.shard_map(
        shards,
        mesh=mesh,
        in_specs=(
            P("ep", None),
            P("ep", None),
            P("ep", None),
            P(),
            P("ep", None, "tp"),
            P("ep", None, "tp"),
            P("ep", "tp", None),
        ),
        out_specs=P("ep", "tp"),
        check_vma=False,
    )
```
